512 devices in a mesh: sp: 64 (over z, y), tp: 8 (over x, core).
Axes of the slice: x: 4, y: 4, z: 16, core: 2. Of those that a mesh axis runs over, the one named last changes fastest.
Arguments:
- residual: bfloat16 [16384, 2048], P('sp'), may hold values from -6 to 6
- queries: bfloat16 [16384, 1024], P('sp', 'tp'), may hold values from -6 to 6
- forget_gate_logits: bfloat16 [16384, 1024], P('sp', 'tp'), may hold values from -5 to 5
- projected_values: bfloat16 [16384, 1024], P('sp', 'tp'), may hold values from -6 to 6
- output_gate_logits: bfloat16 [16384, 1024], P('sp', 'tp'), may hold values from -6 to 6
- lower_bound_margin: float32 [1024], P('tp'), may hold values from 6.1035156e-05 to 0.08
- extra_forget_logs: float32 [16384, 1024], P('sp', 'tp'), may hold values from -0.7 to 0
- per_head_norm_gain: float32 [128], replicated, may hold values from 0.1 to 1.9
- output_weight: bfloat16 [1024, 2048], P('tp'), may hold values from -0.1875 to 0.1875
- feedforward_norm_gain: float32 [2048], replicated, may hold values from 0.1 to 1.9
- gate_weight: bfloat16 [2048, 5632], P('sp', 'tp'), may hold values from -0.125 to 0.125
- up_weight: bfloat16 [2048, 5632], P('sp', 'tp'), may hold values from -0.125 to 0.125
- down_weight: bfloat16 [5632, 2048], P('tp', 'sp'), may hold values from -0.078125 to 0.078125
Outputs:
- layer_out: bfloat16 [16384, 2048], P('sp')
The draws below stay inside these ranges and needn't reach their ends.
All inputs are finite; a program needn't handle non-finite values.
Results may differ from the reference program's by a relative error of at most 0.015.
Values may be sent and summed in bfloat16 or wider, within the bound.
No kernel may reach another device: no remote copies, remote signals or barrier semaphores. Data moves between devices by JAX's collectives and lax.ppermute only.
A program may use at most 64 MiB of HBM per device.

```python
import math
import jax
import jax.numpy as jnp
from jax import lax

D = 2048
FF = 5632
HEADS = 8
HD = 128
HW = 1024
BLOCK = 64
TOK_DEV = 256
SEQ = 16384
N_TP = 8


def draw_lower_bound_margin(key, part):
    order = jax.random.permutation(jax.random.fold_in(key, 1), HEADS)
    slow = order < HEADS // 2
    slow_gap = 2.0 / SEQ * jax.random.uniform(jax.random.fold_in(key, 2), (HEADS, HD), jnp.float32, 0.5, 1.5)
    fast_gap = jnp.exp(jax.random.uniform(jax.random.fold_in(key, 3), (HEADS, HD), jnp.float32, math.log(0.03), math.log(0.08)))
    gaps = jnp.where(slow[:, None], slow_gap, fast_gap)
    return gaps.reshape(HW).astype(jnp.float32)


def draw_forget_gate_logits(key, part):
    base = jnp.clip(jax.random.normal(jax.random.fold_in(key, 1), (SEQ, HW), jnp.float32), -4.0, 4.0)
    shifts = jax.random.uniform(jax.random.fold_in(key, 2), (SEQ // TOK_DEV, 1, HW), jnp.float32, -1.0, 1.0)
    shifted = base.reshape(SEQ // TOK_DEV, TOK_DEV, HW) + shifts
    return shifted.reshape(SEQ, HW).astype(jnp.bfloat16)


def draw_extra_forget_logs(key, part):
    spots = jax.random.randint(jax.random.fold_in(key, 1), (4,), 0, SEQ)
    struck = jnp.any(jnp.arange(SEQ)[:, None] == spots[None, :], axis=1)
    depth = jax.random.uniform(jax.random.fold_in(key, 2), (SEQ, HW), jnp.float32, math.log(0.5), math.log(0.8))
    return jnp.where(struck[:, None], depth, 0.0).astype(jnp.float32)


def steps_of(stream_key, shape, cuts, least, largest):
    gain, own = 1.0, jax.random.fold_in(stream_key, 6)
    for axis_at, blocks in cuts:
        draws = jnp.exp(jax.random.uniform(jax.random.fold_in(own, axis_at), (blocks,), jnp.float32, least / len(cuts), largest / len(cuts)))
        gain = gain * jnp.repeat(draws, shape[axis_at] // blocks).reshape([-1 if axis == axis_at else 1 for axis in range(len(shape))])
    return gain


def centred(stream_key, shape, scale, limit, shards=(), kind=jnp.bfloat16):
    loudness = steps_of(stream_key, shape, shards, -0.22, 0.18) if shards else 1.0
    values = jax.random.normal(stream_key, shape, jnp.float32) * scale * loudness
    return jnp.minimum(jnp.maximum(values, -limit), limit).astype(kind)


def setup_inputs(seed: int = 0) -> dict:
    arg_keys = jax.random.split(jax.random.key(seed), 14)
    return {
        "residual": centred(arg_keys[0], (SEQ, D), 1.0, 6.0, ((0, 64),)),
        "queries": centred(arg_keys[1], (SEQ, HW), 1.0, 6.0, ((0, 64), (1, 8))),
        "forget_gate_logits": draw_forget_gate_logits(jax.random.fold_in(arg_keys[13], 71), 0),
        "projected_values": centred(arg_keys[3], (SEQ, HW), 1.0, 6.0, ((0, 64), (1, 8))),
        "output_gate_logits": centred(arg_keys[4], (SEQ, HW), 1.0, 6.0, ((0, 64), (1, 8))),
        "lower_bound_margin": draw_lower_bound_margin(jax.random.fold_in(arg_keys[13], 71), 0),
        "extra_forget_logs": draw_extra_forget_logs(jax.random.fold_in(arg_keys[13], 71), 0),
        "per_head_norm_gain": jnp.clip(1.0 + 0.18 * jax.random.normal(arg_keys[7], (HD,), jnp.float32), 0.1, 1.9),
        "output_weight": centred(arg_keys[8], (HW, D), HW ** -0.5, 0.1875, ((0, 8),)),
        "feedforward_norm_gain": jnp.clip(1.0 + 0.18 * jax.random.normal(arg_keys[9], (D,), jnp.float32), 0.1, 1.9),
        "gate_weight": centred(arg_keys[10], (D, FF), D ** -0.5, 0.125, ((0, 64), (1, 8))),
        "up_weight": centred(arg_keys[11], (D, FF), D ** -0.5, 0.125, ((0, 64), (1, 8))),
        "down_weight": centred(arg_keys[12], (FF, D), FF ** -0.5, 0.078125, ((0, 8), (1, 64))),
    }


eps = 1e-06
top_precision = lax.Precision.HIGHEST

def block_update(recurrent_state, inputs):
    queries, state_increment, value_rows, retain_log_factor = inputs
    running_state = jnp.cumsum(retain_log_factor, axis=1)
    causal = jnp.tril(jnp.ones((retain_log_factor.shape[1], retain_log_factor.shape[1]), dtype=bool))
    carried_over_state = jnp.einsum('uqw,uwa->uqa', queries * jnp.exp(running_state), recurrent_state, precision=top_precision)
    spread = running_state[:, :, None, :] - running_state[:, None, :, :]
    weights = jnp.exp(jnp.where(causal[None, :, :, None], spread, -jnp.inf))
    scores = jnp.einsum('htk,htsk,hsk->hts', queries, weights, state_increment, precision=top_precision)
    output_rows = carried_over_state + jnp.einsum('hts,hsv->htv', scores, value_rows, precision=top_precision)
    final_state = running_state[:, -1:, :]
    updated_state = jnp.exp(final_state[:, 0, :])[:, :, None] * recurrent_state + jnp.einsum('erb,erc->ebc', state_increment * jnp.exp(final_state - running_state), value_rows, precision=top_precision)
    return (updated_state, output_rows)

def grouped_product(left, right, groups):
    group_width = left.shape[1] // groups
    summed = jnp.zeros((left.shape[0], right.shape[1]), jnp.float32)
    for member in range(groups):
        lower = member * group_width
        upper = lower + group_width
        part_product = jnp.dot(left[:, lower:upper], right[lower:upper], preferred_element_type=jnp.float32)
        rounded = lax.optimization_barrier(part_product.astype(jnp.bfloat16))
        summed = summed + rounded.astype(jnp.float32)
    return summed

def reference(residual, queries, forget_gate_logits, projected_values, output_gate_logits, lower_bound_margin, extra_forget_logs, per_head_norm_gain, output_weight, feedforward_norm_gain, gate_weight, up_weight, down_weight):
    state_increment = lower_bound_margin * jax.nn.sigmoid(-forget_gate_logits.astype(jnp.float32))
    retain_log_factor = jnp.log1p(-state_increment) + extra_forget_logs

    def to_blocks(source):
        return source.reshape(SEQ // BLOCK, BLOCK, HEADS, HD).transpose(0, 2, 1, 3)
    initial = jnp.zeros((HEADS, HD, HD), jnp.float32)
    block_inputs = (to_blocks(queries.astype(jnp.float32)), to_blocks(state_increment), to_blocks(projected_values.astype(jnp.float32)), to_blocks(retain_log_factor))
    _, output_rows = lax.scan(block_update, initial, block_inputs)
    mixed = output_rows.transpose(0, 2, 1, 3).reshape(SEQ, HEADS, HD)
    normed_heads = mixed * lax.rsqrt(lax.optimization_barrier(jnp.mean(mixed * mixed, axis=-1, keepdims=True)) + eps) * per_head_norm_gain
    gating = jax.nn.silu(output_gate_logits.astype(jnp.float32)).reshape(SEQ, HEADS, HD)
    gated = (normed_heads * gating).reshape(SEQ, HW).astype(jnp.bfloat16)
    projected = grouped_product(gated, output_weight, N_TP)
    after_mixer = (residual.astype(jnp.float32) + projected).astype(jnp.bfloat16)
    widened = after_mixer.astype(jnp.float32)
    normed = (widened * lax.rsqrt(lax.optimization_barrier(jnp.mean(widened * widened, axis=-1, keepdims=True)) + eps) * feedforward_norm_gain).astype(jnp.bfloat16)
    group_width = FF // N_TP
    ffn_sum = jnp.zeros((SEQ, D), jnp.float32)
    for member in range(N_TP):
        lower = member * group_width
        upper = lower + group_width
        gate_part = jnp.dot(normed, gate_weight[:, lower:upper], preferred_element_type=jnp.float32)
        up_part = jnp.dot(normed, up_weight[:, lower:upper], preferred_element_type=jnp.float32)
        hidden = (jax.nn.silu(gate_part) * up_part).astype(jnp.bfloat16)
        part_product = jnp.dot(hidden, down_weight[lower:upper], preferred_element_type=jnp.float32)
        rounded = lax.optimization_barrier(part_product.astype(jnp.bfloat16))
        ffn_sum = ffn_sum + rounded.astype(jnp.float32)
    return (after_mixer.astype(jnp.float32) + 0.5 * ffn_sum).astype(jnp.bfloat16)
```

```python
import jax
import jax.numpy as jnp
from jax import lax
from jax.experimental import pallas as pl
from jax.experimental.pallas import tpu as pltpu
from jax.sharding import Mesh
from jax.sharding import PartitionSpec as P

HD = 128
BLOCK = 64
SP = ("z", "y")
TP = ("x", "c")
SCALE = 2.0**18


eps = 1e-06


def nothing_yet(value, identity):
    return jax.tree.map(
        lambda a, e: jnp.broadcast_to(jnp.asarray(e, a.dtype), a.shape), value, identity
    )


def gathered_once(value, axis):
    leaves = jax.tree.leaves(value)
    order = sorted(range(len(leaves)), key=lambda k: -leaves[k].size)
    width = (1, *leaves[order[0]].shape)[-1]
    lines = [
        jnp.pad(leaves[k].reshape(-1), (0, -leaves[k].size % width)).reshape(-1, width)
        for k in order
    ]
    both, at, found = (lax.all_gather(jnp.concatenate(lines), axis), 0, {})
    for k, line in zip(order, lines):
        section = both[:, at : at + len(line)].reshape(len(both), -1)
        found[k] = section[:, : leaves[k].size].reshape(-1, *leaves[k].shape)
        at += len(line)
    numbers = iter(range(len(leaves)))
    return jax.tree.map(lambda _: found[next(numbers)], value)


def carried_in_2(value, axes, combine, identity):
    before = start = nothing_yet(value, identity)
    running = value
    for axis in reversed(axes):
        length, place = (lax.axis_size(axis), lax.axis_index(axis))
        pieces = gathered_once(
            jax.tree.map(
                lambda part, kind: part.astype(kind), running, (jnp.bfloat16, jnp.bfloat16)
            ),
            axis,
        )
        inside, running = (start, start)
        for k in range(length):
            passed = k < place
            running = combine(
                running, jax.tree.map(lambda part, own: part[k].astype(own.dtype), pieces, value)
            )
            inside = jax.tree.map(lambda new, old: jnp.where(passed, new, old), running, inside)
        before = combine(inside, before)
    return before


def block_update(carried_in, inputs):
    recurrent_state, offset = carried_in
    queries, state_increment, value_rows, retain_log_factor = inputs
    running_state = jnp.cumsum(retain_log_factor, axis=1)
    causal = jnp.tril(
        jnp.ones((retain_log_factor.shape[1], retain_log_factor.shape[1]), dtype=bool)
    )
    carried_over_state = jnp.einsum(
        "uqw,uwa->uqa", queries * jnp.exp(running_state), recurrent_state
    )
    spread = running_state[:, :, None, :] - running_state[:, None, :, :]
    weights = jnp.exp(jnp.where(causal[None, :, :, None], spread, -jnp.inf))
    scores = jnp.einsum("htk,htsk,hsk->hts", queries, weights, state_increment)
    output_rows = carried_over_state + jnp.einsum("hts,hsv->htv", scores, value_rows)
    final_state = running_state[:, -1:, :]
    updated_state = jnp.exp(final_state[:, 0, :])[:, :, None] * recurrent_state + jnp.einsum(
        "erb,erc->ebc", state_increment * jnp.exp(final_state - running_state), value_rows
    )
    rescaled_state = queries * jnp.exp(running_state + offset[:, None, :])
    return ((updated_state, offset + final_state[:, 0, :]), (output_rows, rescaled_state))


def join_states(earlier, later):
    earlier_sum, earlier_memory = earlier
    later_sum, later_memory = later
    return (earlier_sum + later_sum, jnp.exp(later_sum)[:, :, None] * earlier_memory + later_memory)


def shifted(value, axis, step):
    size = lax.axis_size(axis)
    return lax.ppermute(value, axis, [(k, (k + step) % size) for k in range(size)])


def ffn_kernel(y_ref, rows_ref, own_ref, down1_ref, up1_ref, low_ref, high_ref, out_ref, weights, hidden):
    y = y_ref[0]
    places = [lax.rem(y + k, 4) for k in range(4)]

    def place(ref, at, z_from, z_to, offset):
        @pl.loop(z_from, z_to)
        def _(z):
            start = pl.multiple_of(z * 128 + at * 32, 32)
            source = pl.multiple_of((z - offset) * 32, 32)
            weights[pl.ds(start, 32), :] = ref[pl.ds(source, 32), :]

    place(own_ref, places[0], 0, 16, 0)
    place(up1_ref, places[1], 0, 16, 0)
    place(down1_ref, places[3], 0, 16, 0)
    place(low_ref, places[2], 0, 8, 0)
    place(high_ref, places[2], 8, 16, 8)
    rows = rows_ref[...]

    @pl.loop(0, 5)
    def _(n):
        gate_at = pl.multiple_of(n * 128, 128)
        up_at = pl.multiple_of(640 + n * 128, 128)
        gate = jnp.dot(rows, weights[:, pl.ds(gate_at, 128)], preferred_element_type=jnp.float32)
        up = jnp.dot(rows, weights[:, pl.ds(up_at, 128)], preferred_element_type=jnp.float32)
        hidden[:, pl.ds(gate_at, 128)] = (gate * jax.nn.sigmoid(gate) * up).astype(jnp.bfloat16)

    both = jnp.dot(rows, weights[:, 1280:1408], preferred_element_type=jnp.float32)
    gate, up = both[:, :64], both[:, 64:]
    hidden[:, 640:704] = (gate * jax.nn.sigmoid(gate) * up).astype(jnp.bfloat16)
    inner = hidden[:, :704]

    @pl.loop(0, 8)
    def _(n):
        at = pl.multiple_of(n * 256, 256)
        part = lax.dot_general(
            inner,
            weights[pl.ds(at, 256), 1408:2112],
            (((1,), (1,)), ((), ())),
            preferred_element_type=jnp.float32,
        )
        out_ref[:, pl.ds(at, 256)] = part.astype(jnp.bfloat16)


def ffn(y, rows, own, down1, up1, low, high):
    vmem = pl.BlockSpec(memory_space=pltpu.VMEM)
    return pl.pallas_call(
        ffn_kernel,
        out_shape=jax.ShapeDtypeStruct((256, 2048), jnp.bfloat16),
        in_specs=[pl.BlockSpec(memory_space=pltpu.SMEM)] + [vmem] * 6,
        out_specs=vmem,
        scratch_shapes=[
            pltpu.VMEM((2048, 2176), jnp.bfloat16),
            pltpu.VMEM((256, 768), jnp.bfloat16),
        ],
        compiler_params=pltpu.CompilerParams(vmem_limit_bytes=50 * 2**20),
        cost_estimate=pl.CostEstimate(
            flops=2 * 256 * 2048 * 2112, bytes_accessed=11 * 2**20, transcendentals=256 * 704
        ),
        name="ffn",
    )(y, rows, own, down1, up1, low, high)


def local(
    residual,
    queries,
    forget_gate_logits,
    projected_values,
    output_gate_logits,
    lower_bound_margin,
    extra_forget_logs,
    per_head_norm_gain,
    output_weight,
    feedforward_norm_gain,
    gate_weight,
    up_weight,
    down_weight,
):
    packed = jnp.concatenate(
        [
            gate_weight[:, :640],
            up_weight[:, :640],
            gate_weight[:, 640:],
            up_weight[:, 640:],
            down_weight.T,
            jnp.zeros((32, 64), jnp.bfloat16),
        ],
        axis=1,
    )
    packed = (packed.astype(jnp.float32) * SCALE).astype(jnp.float16)
    along_z = lax.all_gather(packed, "z", axis=0, tiled=True)
    own = (along_z.astype(jnp.float32) * (1.0 / SCALE)).astype(jnp.bfloat16)
    out_copies = jnp.broadcast_to(output_weight, (8, *output_weight.shape))
    out_full = lax.all_to_all(out_copies, TP, split_axis=0, concat_axis=0, tiled=True)
    out_full = out_full.reshape(1024, 2048)
    down1 = shifted(own, "y", 1)
    up1 = shifted(own, "y", -1)

    length = queries.shape[0]
    head_count = queries.shape[1] // HD
    state_increment = lower_bound_margin * jax.nn.sigmoid(-forget_gate_logits.astype(jnp.float32))
    retain_log_factor = jnp.log1p(-state_increment) + extra_forget_logs

    def to_blocks(source):
        return source.reshape(length // BLOCK, BLOCK, head_count, HD).transpose(0, 2, 1, 3)

    initial = (
        jnp.zeros((head_count, HD, HD), jnp.float32),
        jnp.zeros((head_count, HD), jnp.float32),
    )
    block_inputs = (
        to_blocks(queries.astype(jnp.float32)),
        to_blocks(state_increment),
        to_blocks(projected_values.astype(jnp.float32)),
        to_blocks(retain_log_factor),
    )
    (recurrent_state, decay_sum), (output_rows, rescaled_state) = lax.scan(
        block_update, initial, block_inputs
    )
    identity = (jnp.zeros_like(decay_sum), jnp.zeros_like(recurrent_state))
    incoming_state = carried_in_2((decay_sum, recurrent_state), SP, join_states, identity)[1]
    incoming_state, down1, up1 = lax.optimization_barrier((incoming_state, down1, up1))
    low = shifted(down1[:256], "y", 1)
    high = shifted(up1[256:], "y", -1)
    output_rows = output_rows + jnp.einsum("sjey,jyx->sjex", rescaled_state, incoming_state)
    mixed = output_rows.transpose(0, 2, 1, 3).reshape(length, head_count, HD)
    normed_heads = (
        mixed
        * lax.rsqrt(jnp.mean(mixed * mixed, axis=-1, keepdims=True) + eps)
        * per_head_norm_gain
    )
    gating = jax.nn.silu(output_gate_logits.astype(jnp.float32)).reshape(length, head_count, HD)
    gated = (normed_heads * gating).reshape(length, head_count * HD).astype(jnp.bfloat16)
    gated_all = lax.all_gather(gated, TP)
    gated_all = gated_all.transpose(1, 0, 2).reshape(256, 1024)
    projected = jnp.dot(gated_all, out_full, preferred_element_type=jnp.float32)
    after_mixer = (residual.astype(jnp.float32) + projected).astype(jnp.bfloat16)
    widened = after_mixer.astype(jnp.float32)
    normed = (
        widened
        * lax.rsqrt(jnp.mean(widened * widened, axis=-1, keepdims=True) + eps)
        * feedforward_norm_gain
    ).astype(jnp.bfloat16)
    y = lax.axis_index("y").reshape(1)
    part = ffn(y, normed, own, down1, up1, low, high)

    core = lax.axis_index("c")
    part = part.reshape(4, 2, 32, 2048)
    theirs = lax.dynamic_index_in_dim(part, 1 - core, 1, keepdims=False)
    mine = lax.dynamic_index_in_dim(part, core, 1, keepdims=False)
    swapped = shifted(theirs, "c", 1)
    pair = (mine.astype(jnp.float32) + swapped.astype(jnp.float32)).astype(jnp.bfloat16)
    arrived = lax.all_to_all(pair, "x", split_axis=0, concat_axis=0, tiled=True)
    ffn_sum = arrived.astype(jnp.float32).sum(axis=0)
    place = lax.axis_index(TP) * 32
    own_rows = lax.dynamic_slice_in_dim(after_mixer, place, 32, 0)
    finished = (own_rows.astype(jnp.float32) + 0.5 * ffn_sum).astype(jnp.bfloat16)
    along_x = lax.all_gather(finished, "x")
    others = shifted(along_x, "c", 1)
    first = jnp.where(core == 0, along_x, others)
    second = jnp.where(core == 0, others, along_x)
    return jnp.stack([first, second], axis=1).reshape(256, 2048)


def solution(mesh):
    finer = Mesh(mesh.devices.reshape(16, 4, 4, 2), ("z", "y", "x", "c"))
    placed = (
        P(SP, None),
        P(SP, TP),
        P(SP, TP),
        P(SP, TP),
        P(SP, TP),
        P(TP),
        P(SP, TP),
        P(),
        P(TP, None),
        P(),
        P(SP, TP),
        P(SP, TP),
        P(TP, SP),
    )
    return jax.shard_map(local, mesh=finer, in_specs=placed, out_specs=P(SP, None), check_vma=False)
```

```python
import jax
import jax.numpy as jnp
from jax import lax
from jax.experimental import pallas as pl
from jax.experimental.pallas import tpu as pltpu
from jax.sharding import Mesh
from jax.sharding import PartitionSpec as P

HD = 128
BLOCK = 64
SP = ("z", "y")
TP = ("x", "c")
SCALE = 2.0**18
STATE_SCALE = 2.0**10
NN = (((1,), (0,)), ((), ()))
NT = (((1,), (1,)), ((), ()))
TN = (((0,), (0,)), ((), ()))


eps = 1e-06


def shifted(value, axis, step):
    size = lax.axis_size(axis)
    return lax.ppermute(value, axis, [(k, (k + step) % size) for k in range(size)])


def whole(space=pltpu.VMEM):
    return pl.BlockSpec(memory_space=space)


def dot(left, right, dims=NN):
    return lax.dot_general(
        left.astype(jnp.bfloat16),
        right.astype(jnp.bfloat16),
        dims,
        preferred_element_type=jnp.float32,
    )


def scan_kernel(q_ref, f_ref, v_ref, margin_ref, extra_ref, out_ref, scaled_ref, lines_ref):
    queries = q_ref[...].astype(jnp.float32)
    inflow = margin_ref[...] * jax.nn.sigmoid(-f_ref[...].astype(jnp.float32))
    keep_log = jnp.log1p(-inflow) + extra_ref[...]
    row = lax.broadcasted_iota(jnp.int32, (256, 256), 0)
    column = lax.broadcasted_iota(jnp.int32, (256, 256), 1)
    lower = (column <= row).astype(jnp.float32)
    total = jnp.dot(
        lower, keep_log, precision=lax.Precision.HIGHEST, preferred_element_type=jnp.float32
    )
    scaled_ref[...] = (queries * jnp.exp(total)).astype(jnp.bfloat16)
    causal = lax.broadcasted_iota(jnp.int32, (BLOCK, BLOCK), 1) <= lax.broadcasted_iota(
        jnp.int32, (BLOCK, BLOCK), 0
    )
    state = None
    ended = jnp.zeros((1, HD), jnp.float32)
    for k in range(256 // BLOCK):
        rows = slice(k * BLOCK, (k + 1) * BLOCK)
        inside, sums = queries[rows], total[rows]
        middle, end = sums[BLOCK // 2 - 1 : BLOCK // 2], sums[BLOCK - 1 :]
        values = v_ref[rows]
        scores = dot(inside * jnp.exp(sums - middle), inflow[rows] * jnp.exp(middle - sums), NT)
        result = dot(jnp.where(causal, scores, 0.0), values)
        added = dot(values, inflow[rows] * jnp.exp(end - sums), TN)
        if state is not None:
            result = result + dot(inside * jnp.exp(sums - ended), state, NT)
            added = added + jnp.exp(end - ended) * state
        out_ref[rows, :] = result
        state, ended = added, end
    packed = state.astype(jnp.bfloat16)
    for k in range(8):
        lines_ref[:, k * 128 : (k + 1) * 128] = packed[k * 16 : (k + 1) * 16]
    lines_ref[:, 1024:1152] = jnp.broadcast_to(ended, (16, HD)).astype(jnp.bfloat16)
    lines_ref[:, 1152:1280] = jnp.zeros((16, HD), jnp.bfloat16)


def scanned(queries, logits, values, margin, extra):
    return pl.pallas_call(
        scan_kernel,
        out_shape=(
            jax.ShapeDtypeStruct((256, HD), jnp.float32),
            jax.ShapeDtypeStruct((256, HD), jnp.bfloat16),
            jax.ShapeDtypeStruct((16, 1280), jnp.bfloat16),
        ),
        in_specs=[whole()] * 5,
        out_specs=(whole(),) * 3,
        cost_estimate=pl.CostEstimate(
            flops=4_000_000_000, bytes_accessed=500_000, transcendentals=300_000
        ),
        name="scan",
    )(queries, logits, values, margin, extra)


def y_kernel(y_ref, pieces_ref, total_ref, here_ref):
    y = y_ref[0]
    total_sum = here_sum = jnp.zeros((1, HD), jnp.float32)
    total = here = jnp.zeros((HD, HD), jnp.float32)
    for k in range(4):
        here = jnp.where(k == y, total, here)
        here_sum = jnp.where(k == y, total_sum, here_sum)
        state = jnp.concatenate(
            [pieces_ref[k, 32:48, j * 128 : (j + 1) * 128] for j in range(8)], axis=0
        ).astype(jnp.float32)
        one = pieces_ref[k, 32:48, 1024:1152].astype(jnp.float32)[:1]
        total = jnp.exp(one) * total + state
        total_sum = total_sum + one
    here_ref[:HD, :] = here
    here_ref[HD:, :] = jnp.broadcast_to(here_sum, (8, HD))
    lines = jnp.concatenate(
        [total * STATE_SCALE, jnp.broadcast_to(total_sum, (40, HD))], axis=0
    )
    for j in range(7):
        total_ref[:, j * 128 : (j + 1) * 128] = lines[j * 24 : (j + 1) * 24]


def joined_over_y(y, pieces):
    return pl.pallas_call(
        y_kernel,
        out_shape=(
            jax.ShapeDtypeStruct((24, 896), jnp.float32),
            jax.ShapeDtypeStruct((136, HD), jnp.float32),
        ),
        in_specs=[whole(pltpu.SMEM), whole()],
        out_specs=(whole(), whole()),
        cost_estimate=pl.CostEstimate(
            flops=1_000_000_000, bytes_accessed=700_000, transcendentals=1000
        ),
        name="join",
    )(y, pieces)


def mix_kernel(z_ref, lines_ref, here_ref, out_ref, scaled_ref, logits_ref, gain_ref, gated_ref):
    z = z_ref[0]
    before = jnp.zeros((HD, HD), jnp.float32)
    for k in range(15):
        lines = jnp.concatenate(
            [lines_ref[k, :, j * 128 : (j + 1) * 128] for j in range(7)], axis=0
        )
        joined = jnp.exp(lines[HD : HD + 1]) * before + lines[:HD]
        before = jnp.where(k < z, joined, before)
    here = here_ref[...]
    state = jnp.exp(here[HD : HD + 1]) * (before * (1.0 / STATE_SCALE)) + here[:HD]
    mixed = out_ref[...] + dot(scaled_ref[...], state, NT)
    normed = mixed * lax.rsqrt(jnp.mean(mixed * mixed, axis=-1, keepdims=True) + eps)
    logits = logits_ref[...].astype(jnp.float32)
    gated_ref[...] = (normed * gain_ref[...] * (logits * jax.nn.sigmoid(logits))).astype(
        jnp.bfloat16
    )


def mixed_rows(z, lines, here, out, scaled, logits, gain):
    return pl.pallas_call(
        mix_kernel,
        out_shape=jax.ShapeDtypeStruct((256, HD), jnp.bfloat16),
        in_specs=[whole(pltpu.SMEM)] + [whole()] * 6,
        out_specs=whole(),
        cost_estimate=pl.CostEstimate(
            flops=2_000_000_000, bytes_accessed=2_000_000, transcendentals=100_000
        ),
        name="mix",
    )(z, lines, here, out, scaled, logits, gain)


def ffn_kernel(
    y_ref,
    rows_ref,
    wide_ref,
    own_ref,
    down1_ref,
    up1_ref,
    low_ref,
    high_ref,
    out_ref,
    columns,
    weights,
    hidden,
    column_sems,
    piece_sems,
):
    y = y_ref[0]
    places = [lax.rem(y + k, 4) for k in range(4)]
    column_copies = [
        pltpu.make_async_copy(
            wide_ref.at[:, pl.ds(n * 128, 128)], columns.at[n], column_sems.at[n]
        )
        for n in range(10)
    ]
    piece_copies = [
        pltpu.make_async_copy(ref, weights.at[pl.ds(start, size), places[k]], piece_sems.at[n])
        for n, (ref, k, start, size) in enumerate(
            (
                (own_ref, 0, 0, 16),
                (up1_ref, 1, 0, 16),
                (down1_ref, 3, 0, 16),
                (low_ref, 2, 0, 8),
                (high_ref, 2, 8, 8),
            )
        )
    ]
    for n in range(5):
        column_copies[n].start()
        column_copies[n + 5].start()
    for copy in piece_copies:
        copy.start()
    rows = rows_ref[...]

    for n in range(5):
        column_copies[n].wait()
        gate = jnp.dot(rows, columns[n], preferred_element_type=jnp.float32)
        column_copies[n + 5].wait()
        up = jnp.dot(rows, columns[n + 5], preferred_element_type=jnp.float32)
        hidden[:, n * 128 : (n + 1) * 128] = (gate * jax.nn.sigmoid(gate) * up).astype(
            jnp.bfloat16
        )
    for copy in piece_copies:
        copy.wait()
    last = weights[:, :, :, :128].reshape(2048, 128)
    both = jnp.dot(rows, last, preferred_element_type=jnp.float32)
    gate, up = both[:, :64], both[:, 64:]
    hidden[:, 640:704] = (gate * jax.nn.sigmoid(gate) * up).astype(jnp.bfloat16)
    inner = hidden[:, :704]

    @pl.loop(0, 8)
    def _(n):
        at = pl.multiple_of(n * 256, 256)
        part = lax.dot_general(
            inner,
            weights[pl.ds(n * 2, 2), :, :, 128:832].reshape(256, 704),
            NT,
            preferred_element_type=jnp.float32,
        )
        out_ref[:, pl.ds(at, 256)] = part.astype(jnp.bfloat16)


def ffn(y, rows, wide, *pieces):
    pieces = [piece.reshape(-1, 32, 896) for piece in pieces]
    return pl.pallas_call(
        ffn_kernel,
        out_shape=jax.ShapeDtypeStruct((256, 2048), jnp.bfloat16),
        in_specs=[whole(pltpu.SMEM), whole()] + [whole(pltpu.HBM)] * 6,
        out_specs=whole(),
        scratch_shapes=[
            pltpu.VMEM((10, 2048, 128), jnp.bfloat16),
            pltpu.VMEM((16, 4, 32, 896), jnp.bfloat16),
            pltpu.VMEM((256, 768), jnp.bfloat16),
            pltpu.SemaphoreType.DMA((10,)),
            pltpu.SemaphoreType.DMA((5,)),
        ],
        compiler_params=pltpu.CompilerParams(vmem_limit_bytes=32 * 2**20),
        cost_estimate=pl.CostEstimate(
            flops=2 * 256 * 2048 * 2112, bytes_accessed=11 * 2**20, transcendentals=256 * 704
        ),
        name="ffn",
    )(y, rows, wide, *pieces)


def local(
    residual,
    queries,
    forget_gate_logits,
    projected_values,
    output_gate_logits,
    lower_bound_margin,
    extra_forget_logs,
    per_head_norm_gain,
    output_weight,
    feedforward_norm_gain,
    gate_weight,
    up_weight,
    down_weight,
):
    y = lax.axis_index("y").reshape(1)
    z = lax.axis_index("z").reshape(1)
    with jax.named_scope("outgather"):
        out_copies = jnp.broadcast_to(output_weight, (8, *output_weight.shape))
        out_full = lax.all_to_all(out_copies, TP, split_axis=0, concat_axis=0, tiled=True)
        out_full = out_full.reshape(1024, 2048)
    by_y = jnp.concatenate([gate_weight[:, :640], up_weight[:, :640]], axis=1)
    by_z = jnp.concatenate(
        [gate_weight[:, 640:], up_weight[:, 640:], down_weight.T, jnp.zeros((32, 64), jnp.bfloat16)],
        axis=1,
    )
    by_z = (by_z.astype(jnp.float32) * SCALE).astype(jnp.float16)
    out_rows, scaled, lines = scanned(
        queries,
        forget_gate_logits,
        projected_values,
        lower_bound_margin.reshape(1, HD),
        extra_forget_logs,
    )
    with jax.named_scope("ygather"):
        along_y = lax.all_gather(jnp.concatenate([by_y, lines], axis=0), "y")
    with jax.named_scope("widegather"):
        wide = lax.all_gather(along_y[:, :32].reshape(128, 1280), "z", axis=0, tiled=True)
    total, here = joined_over_y(y, along_y)
    with jax.named_scope("zgather"):
        along_z = lax.all_gather(
            jnp.concatenate([by_z, total.astype(jnp.float16)], axis=0), "z"
        )
    own = (along_z[:, :32].astype(jnp.float32) * (1.0 / SCALE)).astype(jnp.bfloat16)
    own = own.reshape(512, 896)
    down1 = shifted(own, "y", 1)
    up1 = shifted(own, "y", -1)
    gated = mixed_rows(
        z,
        along_z[:, 32:].astype(jnp.float32),
        here,
        out_rows,
        scaled,
        output_gate_logits,
        per_head_norm_gain.reshape(1, HD),
    )
    with jax.named_scope("gatedgather"):
        gated_all = lax.all_gather(gated, TP)
    gated_all, down1, up1 = lax.optimization_barrier((gated_all, down1, up1))
    low = shifted(down1[:256], "y", 1)
    high = shifted(up1[256:], "y", -1)
    gated_all = gated_all.transpose(1, 0, 2).reshape(256, 1024)
    projected = jnp.dot(gated_all, out_full, preferred_element_type=jnp.float32)
    after_mixer = (residual.astype(jnp.float32) + projected).astype(jnp.bfloat16)
    widened = after_mixer.astype(jnp.float32)
    normed = (
        widened
        * lax.rsqrt(jnp.mean(widened * widened, axis=-1, keepdims=True) + eps)
        * feedforward_norm_gain
    ).astype(jnp.bfloat16)
    part = ffn(y, normed, wide, own, down1, up1, low, high)

    core = lax.axis_index("c")
    part = part.reshape(4, 2, 32, 2048)
    theirs = lax.dynamic_index_in_dim(part, 1 - core, 1, keepdims=False)
    mine = lax.dynamic_index_in_dim(part, core, 1, keepdims=False)
    swapped = shifted(theirs, "c", 1)
    pair = (mine.astype(jnp.float32) + swapped.astype(jnp.float32)).astype(jnp.bfloat16)
    place = lax.axis_index(TP) * 32
    own_rows = lax.dynamic_slice_in_dim(after_mixer, place, 32, 0)
    pair, own_rows = lax.optimization_barrier((pair, own_rows))
    arrived = lax.all_to_all(pair, "x", split_axis=0, concat_axis=0, tiled=True)
    ffn_sum = arrived.astype(jnp.float32).sum(axis=0)
    finished = (own_rows.astype(jnp.float32) + 0.5 * ffn_sum).astype(jnp.bfloat16)
    along_x = lax.all_gather(finished, "x")
    others = shifted(along_x, "c", 1)
    first = jnp.where(core == 0, along_x, others)
    second = jnp.where(core == 0, others, along_x)
    return jnp.stack([first, second], axis=1).reshape(256, 2048)


def solution(mesh):
    finer = Mesh(mesh.devices.reshape(16, 4, 4, 2), ("z", "y", "x", "c"))
    placed = (
        P(SP, None),
        P(SP, TP),
        P(SP, TP),
        P(SP, TP),
        P(SP, TP),
        P(TP),
        P(SP, TP),
        P(),
        P(TP, None),
        P(),
        P(SP, TP),
        P(SP, TP),
        P(TP, SP),
    )
    return jax.shard_map(local, mesh=finer, in_specs=placed, out_specs=P(SP, None), check_vma=False)
```

```python
import jax
import jax.numpy as jnp
from jax import lax
from jax.experimental import pallas as pl
from jax.experimental.pallas import tpu as pltpu
from jax.sharding import Mesh
from jax.sharding import PartitionSpec as P

HD = 128
BLOCK = 64
SP = ("z", "y")
TP = ("x", "c")
NN = (((1,), (0,)), ((), ()))
NT = (((1,), (1,)), ((), ()))
TN = (((0,), (0,)), ((), ()))


eps = 1e-06


def shifted(value, axis, step):
    size = lax.axis_size(axis)
    return lax.ppermute(value, axis, [(k, (k + step) % size) for k in range(size)])


def whole(space=pltpu.VMEM):
    return pl.BlockSpec(memory_space=space)


def dot(left, right, dims=NN):
    return lax.dot_general(
        left.astype(jnp.bfloat16),
        right.astype(jnp.bfloat16),
        dims,
        preferred_element_type=jnp.float32,
    )


def halves(value):
    high = value.astype(jnp.bfloat16)
    return high, (value - high.astype(jnp.float32)).astype(jnp.bfloat16)


def scan_kernel(q_ref, f_ref, v_ref, margin_ref, extra_ref, out_ref, scaled_ref, lines_ref):
    queries = q_ref[...].astype(jnp.float32)
    inflow = margin_ref[...] * jax.nn.sigmoid(-f_ref[...].astype(jnp.float32))
    keep_log = jnp.log1p(-inflow) + extra_ref[...]
    row = lax.broadcasted_iota(jnp.int32, (256, 256), 0)
    column = lax.broadcasted_iota(jnp.int32, (256, 256), 1)
    lower = (column <= row).astype(jnp.float32)
    total = jnp.dot(
        lower, keep_log, precision=lax.Precision.HIGHEST, preferred_element_type=jnp.float32
    )
    scaled_ref[...] = (queries * jnp.exp(total)).astype(jnp.bfloat16)
    causal = lax.broadcasted_iota(jnp.int32, (BLOCK, BLOCK), 1) <= lax.broadcasted_iota(
        jnp.int32, (BLOCK, BLOCK), 0
    )
    state = None
    ended = jnp.zeros((1, HD), jnp.float32)
    for k in range(256 // BLOCK):
        rows = slice(k * BLOCK, (k + 1) * BLOCK)
        inside, sums = queries[rows], total[rows]
        middle, end = sums[BLOCK // 2 - 1 : BLOCK // 2], sums[BLOCK - 1 :]
        values = v_ref[rows]
        scores = dot(inside * jnp.exp(sums - middle), inflow[rows] * jnp.exp(middle - sums), NT)
        result = dot(jnp.where(causal, scores, 0.0), values)
        added = dot(values, inflow[rows] * jnp.exp(end - sums), TN)
        if state is not None:
            result = result + dot(inside * jnp.exp(sums - ended), state, NT)
            added = added + jnp.exp(end - ended) * state
        out_ref[rows, :] = result
        state, ended = added, end
    packed = state.astype(jnp.bfloat16)
    for k in range(8):
        lines_ref[:, k * 128 : (k + 1) * 128] = packed[k * 16 : (k + 1) * 16]
    high, low = halves(jnp.broadcast_to(ended, (16, HD)))
    lines_ref[:, 1024:1152] = high
    lines_ref[:, 1152:1280] = low


def scanned(queries, logits, values, margin, extra):
    return pl.pallas_call(
        scan_kernel,
        out_shape=(
            jax.ShapeDtypeStruct((256, HD), jnp.float32),
            jax.ShapeDtypeStruct((256, HD), jnp.bfloat16),
            jax.ShapeDtypeStruct((16, 1280), jnp.bfloat16),
        ),
        in_specs=[whole()] * 5,
        out_specs=(whole(),) * 3,
        cost_estimate=pl.CostEstimate(
            flops=4_000_000_000, bytes_accessed=500_000, transcendentals=300_000
        ),
        name="scan",
    )(queries, logits, values, margin, extra)


def y_kernel(y_ref, pieces_ref, total_ref, here_ref):
    y = y_ref[0]
    total_sum = here_sum = jnp.zeros((1, HD), jnp.float32)
    total = here = jnp.zeros((HD, HD), jnp.float32)
    for k in range(4):
        here = jnp.where(k == y, total, here)
        here_sum = jnp.where(k == y, total_sum, here_sum)
        state = jnp.concatenate(
            [pieces_ref[k, :, j * 128 : (j + 1) * 128] for j in range(8)], axis=0
        ).astype(jnp.float32)
        one = pieces_ref[k, :, 1024:1152].astype(jnp.float32)[:1]
        one = one + pieces_ref[k, :, 1152:1280].astype(jnp.float32)[:1]
        total = jnp.exp(one) * total + state
        total_sum = total_sum + one
    here_ref[:HD, :] = here
    here_ref[HD:, :] = jnp.broadcast_to(here_sum, (8, HD))
    packed = total.astype(jnp.bfloat16)
    high, low = halves(jnp.broadcast_to(total_sum, (16, HD)))
    total_ref[:, :128] = packed[:48]
    total_ref[:, 128:256] = packed[48:96]
    total_ref[:32, 256:] = packed[96:]
    row = lax.broadcasted_iota(jnp.int32, (16, HD), 0)
    total_ref[32:, 256:] = jnp.where(row < 8, high, low)


def joined_over_y(y, pieces):
    return pl.pallas_call(
        y_kernel,
        out_shape=(
            jax.ShapeDtypeStruct((48, 384), jnp.bfloat16),
            jax.ShapeDtypeStruct((136, HD), jnp.float32),
        ),
        in_specs=[whole(pltpu.SMEM), whole()],
        out_specs=(whole(), whole()),
        cost_estimate=pl.CostEstimate(
            flops=1_000_000_000, bytes_accessed=700_000, transcendentals=1000
        ),
        name="join",
    )(y, pieces)


def mix_kernel(z_ref, lines_ref, here_ref, out_ref, scaled_ref, logits_ref, gain_ref, gated_ref):
    z = z_ref[0]
    before = jnp.zeros((HD, HD), jnp.float32)
    for k in range(15):
        lines = jnp.concatenate(
            [lines_ref[k, 32:, j * 128 : (j + 1) * 128] for j in range(3)], axis=0
        ).astype(jnp.float32)
        one = lines[HD : HD + 1] + lines[HD + 8 : HD + 9]
        joined = jnp.exp(one) * before + lines[:HD]
        before = jnp.where(k < z, joined, before)
    here = here_ref[...]
    state = jnp.exp(here[HD : HD + 1]) * before + here[:HD]
    mixed = out_ref[...] + dot(scaled_ref[...], state, NT)
    normed = mixed * lax.rsqrt(jnp.mean(mixed * mixed, axis=-1, keepdims=True) + eps)
    logits = logits_ref[...].astype(jnp.float32)
    gated_ref[...] = (normed * gain_ref[...] * (logits * jax.nn.sigmoid(logits))).astype(
        jnp.bfloat16
    )


def mixed_rows(z, lines, here, out, scaled, logits, gain):
    return pl.pallas_call(
        mix_kernel,
        out_shape=jax.ShapeDtypeStruct((256, HD), jnp.bfloat16),
        in_specs=[whole(pltpu.SMEM)] + [whole()] * 6,
        out_specs=whole(),
        cost_estimate=pl.CostEstimate(
            flops=2_000_000_000, bytes_accessed=2_000_000, transcendentals=100_000
        ),
        name="mix",
    )(z, lines, here, out, scaled, logits, gain)


def ffn_kernel(
    y_ref,
    rows_ref,
    wide_ref,
    own_ref,
    down1_ref,
    up1_ref,
    low_ref,
    high_ref,
    out_ref,
    columns,
    rest,
    weights,
    hidden,
    column_sems,
    piece_sems,
):
    y = y_ref[0]
    places = [lax.rem(y + k, 4) for k in range(4)]
    column_copies = [
        pltpu.make_async_copy(
            wide_ref.at[:, pl.ds(n * 256, 256)], columns.at[n], column_sems.at[n]
        )
        for n in range(5)
    ]
    rest_copy = pltpu.make_async_copy(wide_ref.at[:, pl.ds(1280, 512)], rest, column_sems.at[5])
    piece_copies = [
        pltpu.make_async_copy(ref, weights.at[pl.ds(start, size), places[k]], piece_sems.at[n])
        for n, (ref, k, start, size) in enumerate(
            (
                (own_ref, 0, 0, 16),
                (up1_ref, 1, 0, 16),
                (down1_ref, 3, 0, 16),
                (low_ref, 2, 0, 8),
                (high_ref, 2, 8, 8),
            )
        )
    ]
    for copy in column_copies:
        copy.start()
    rest_copy.start()
    for copy in piece_copies:
        copy.start()
    rows = rows_ref[...]

    for n in range(5):
        column_copies[n].wait()
        both = jnp.dot(rows, columns[n], preferred_element_type=jnp.float32)
        gate, up = both[:, :128], both[:, 128:]
        hidden[:, n * 128 : (n + 1) * 128] = (gate * jax.nn.sigmoid(gate) * up).astype(
            jnp.bfloat16
        )
    rest_copy.wait()
    both = jnp.dot(rows, rest[:, :128], preferred_element_type=jnp.float32)
    gate, up = both[:, :64], both[:, 64:]
    hidden[:, 640:704] = (gate * jax.nn.sigmoid(gate) * up).astype(jnp.bfloat16)
    for copy in piece_copies:
        copy.wait()
    first, second = hidden[:, :384], hidden[:, 384:704]

    @pl.loop(0, 8)
    def _(n):
        at = pl.multiple_of(n * 256, 256)
        part = lax.dot_general(
            first,
            weights[pl.ds(n * 2, 2)].reshape(256, 384),
            NT,
            preferred_element_type=jnp.float32,
        ) + lax.dot_general(
            second,
            rest[pl.ds(at, 256), 128:448],
            NT,
            preferred_element_type=jnp.float32,
        )
        out_ref[:, pl.ds(at, 256)] = part.astype(jnp.bfloat16)


def ffn(y, rows, wide, *pieces):
    pieces = [piece.reshape(-1, 32, 384) for piece in pieces]
    return pl.pallas_call(
        ffn_kernel,
        out_shape=jax.ShapeDtypeStruct((256, 2048), jnp.bfloat16),
        in_specs=[whole(pltpu.SMEM), whole()] + [whole(pltpu.HBM)] * 6,
        out_specs=whole(),
        scratch_shapes=[
            pltpu.VMEM((5, 2048, 256), jnp.bfloat16),
            pltpu.VMEM((2048, 512), jnp.bfloat16),
            pltpu.VMEM((16, 4, 32, 384), jnp.bfloat16),
            pltpu.VMEM((256, 768), jnp.bfloat16),
            pltpu.SemaphoreType.DMA((6,)),
            pltpu.SemaphoreType.DMA((5,)),
        ],
        compiler_params=pltpu.CompilerParams(vmem_limit_bytes=60 * 2**20),
        cost_estimate=pl.CostEstimate(
            flops=2 * 256 * 2048 * 2112, bytes_accessed=11 * 2**20, transcendentals=256 * 704
        ),
        name="ffn",
    )(y, rows, wide, *pieces)


def local(
    residual,
    queries,
    forget_gate_logits,
    projected_values,
    output_gate_logits,
    lower_bound_margin,
    extra_forget_logs,
    per_head_norm_gain,
    output_weight,
    feedforward_norm_gain,
    gate_weight,
    up_weight,
    down_weight,
):
    y = lax.axis_index("y").reshape(1)
    z = lax.axis_index("z").reshape(1)
    with jax.named_scope("outgather"):
        out_copies = jnp.broadcast_to(output_weight, (8, *output_weight.shape))
        out_full = lax.all_to_all(out_copies, TP, split_axis=0, concat_axis=0, tiled=True)
        out_full = out_full.reshape(1024, 2048)
    turned = down_weight.T
    blocks = [part[:, n * 128 : (n + 1) * 128] for n in range(5) for part in (gate_weight, up_weight)]
    by_y = jnp.concatenate(
        [
            *blocks,
            gate_weight[:, 640:],
            up_weight[:, 640:],
            turned[:, 384:],
            jnp.zeros((32, 64), jnp.bfloat16),
        ],
        axis=1,
    )
    with jax.named_scope("wideygather"):
        along_y = lax.all_gather(by_y, "y", axis=0, tiled=True)
    with jax.named_scope("widegather"):
        wide = lax.all_gather(along_y, "z", axis=0, tiled=True)
    extra_forget_logs, along_y = lax.optimization_barrier((extra_forget_logs, along_y))
    out_rows, scaled, lines = scanned(
        queries,
        forget_gate_logits,
        projected_values,
        lower_bound_margin.reshape(1, HD),
        extra_forget_logs,
    )
    with jax.named_scope("ygather"):
        states = lax.all_gather(lines, "y")
    total, here = joined_over_y(y, states)
    with jax.named_scope("zgather"):
        along_z = lax.all_gather(jnp.concatenate([turned[:, :384], total], axis=0), "z")
    own = along_z[:, :32].reshape(512, 384)
    down1 = shifted(own, "y", 1)
    up1 = shifted(own, "y", -1)
    gated = mixed_rows(
        z,
        along_z,
        here,
        out_rows,
        scaled,
        output_gate_logits,
        per_head_norm_gain.reshape(1, HD),
    )
    with jax.named_scope("gatedgather"):
        gated_all = lax.all_gather(gated, TP)
    gated_all, down1, up1 = lax.optimization_barrier((gated_all, down1, up1))
    low = shifted(down1[:256], "y", 1)
    high = shifted(up1[256:], "y", -1)
    gated_all = gated_all.transpose(1, 0, 2).reshape(256, 1024)
    projected = jnp.dot(gated_all, out_full, preferred_element_type=jnp.float32)
    after_mixer = (residual.astype(jnp.float32) + projected).astype(jnp.bfloat16)
    widened = after_mixer.astype(jnp.float32)
    normed = (
        widened
        * lax.rsqrt(jnp.mean(widened * widened, axis=-1, keepdims=True) + eps)
        * feedforward_norm_gain
    ).astype(jnp.bfloat16)
    part = ffn(y, normed, wide, own, down1, up1, low, high)

    core = lax.axis_index("c")
    part = part.reshape(4, 2, 32, 2048)
    theirs = lax.dynamic_index_in_dim(part, 1 - core, 1, keepdims=False)
    mine = lax.dynamic_index_in_dim(part, core, 1, keepdims=False)
    swapped = shifted(theirs, "c", 1)
    pair = (mine.astype(jnp.float32) + swapped.astype(jnp.float32)).astype(jnp.bfloat16)
    place = lax.axis_index(TP) * 32
    own_rows = lax.dynamic_slice_in_dim(after_mixer, place, 32, 0)
    pair, own_rows = lax.optimization_barrier((pair, own_rows))
    arrived = lax.all_to_all(pair, "x", split_axis=0, concat_axis=0, tiled=True)
    ffn_sum = arrived.astype(jnp.float32).sum(axis=0)
    finished = (own_rows.astype(jnp.float32) + 0.5 * ffn_sum).astype(jnp.bfloat16)
    along_x = lax.all_gather(finished, "x")
    others = shifted(along_x, "c", 1)
    first = jnp.where(core == 0, along_x, others)
    second = jnp.where(core == 0, others, along_x)
    return jnp.stack([first, second], axis=1).reshape(256, 2048)


def solution(mesh):
    finer = Mesh(mesh.devices.reshape(16, 4, 4, 2), ("z", "y", "x", "c"))
    placed = (
        P(SP, None),
        P(SP, TP),
        P(SP, TP),
        P(SP, TP),
        P(SP, TP),
        P(TP),
        P(SP, TP),
        P(),
        P(TP, None),
        P(),
        P(SP, TP),
        P(SP, TP),
        P(TP, SP),
    )
    return jax.shard_map(local, mesh=finer, in_specs=placed, out_specs=P(SP, None), check_vma=False)
```

```python
import jax
import jax.numpy as jnp
from jax import lax
from jax.experimental import pallas as pl
from jax.experimental.pallas import tpu as pltpu
from jax.sharding import Mesh
from jax.sharding import PartitionSpec as P

HD = 128
BLOCK = 64
SP = ("z", "y")
TP = ("x", "c")
SCALE = 2.0**18
STATE_SCALE = 2.0**10
NN = (((1,), (0,)), ((), ()))
NT = (((1,), (1,)), ((), ()))
TN = (((0,), (0,)), ((), ()))


eps = 1e-06


def shifted(value, axis, step):
    size = lax.axis_size(axis)
    return lax.ppermute(value, axis, [(k, (k + step) % size) for k in range(size)])


def whole(space=pltpu.VMEM):
    return pl.BlockSpec(memory_space=space)


def dot(left, right, dims=NN):
    return lax.dot_general(
        left.astype(jnp.bfloat16),
        right.astype(jnp.bfloat16),
        dims,
        preferred_element_type=jnp.float32,
    )


def halves(value):
    high = value.astype(jnp.bfloat16)
    return high, (value - high.astype(jnp.float32)).astype(jnp.bfloat16)


def scan_kernel(
    q_ref,
    f_ref,
    v_ref,
    margin_ref,
    extra_ref,
    gate_ref,
    up_ref,
    turned_ref,
    out_ref,
    scaled_ref,
    packed_ref,
):
    queries = q_ref[...].astype(jnp.float32)
    inflow = margin_ref[...] * jax.nn.sigmoid(-f_ref[...].astype(jnp.float32))
    keep_log = jnp.log1p(-inflow) + extra_ref[...]
    row = lax.broadcasted_iota(jnp.int32, (256, 256), 0)
    column = lax.broadcasted_iota(jnp.int32, (256, 256), 1)
    lower = (column <= row).astype(jnp.float32)
    total = jnp.dot(
        lower, keep_log, precision=lax.Precision.HIGHEST, preferred_element_type=jnp.float32
    )
    scaled_ref[...] = (queries * jnp.exp(total)).astype(jnp.bfloat16)
    causal = lax.broadcasted_iota(jnp.int32, (BLOCK, BLOCK), 1) <= lax.broadcasted_iota(
        jnp.int32, (BLOCK, BLOCK), 0
    )
    state = None
    ended = jnp.zeros((1, HD), jnp.float32)
    for k in range(256 // BLOCK):
        rows = slice(k * BLOCK, (k + 1) * BLOCK)
        inside, sums = queries[rows], total[rows]
        middle, end = sums[BLOCK // 2 - 1 : BLOCK // 2], sums[BLOCK - 1 :]
        values = v_ref[rows]
        scores = dot(inside * jnp.exp(sums - middle), inflow[rows] * jnp.exp(middle - sums), NT)
        result = dot(jnp.where(causal, scores, 0.0), values)
        added = dot(values, inflow[rows] * jnp.exp(end - sums), TN)
        if state is not None:
            result = result + dot(inside * jnp.exp(sums - ended), state, NT)
            added = added + jnp.exp(end - ended) * state
        out_ref[rows, :] = result
        state, ended = added, end
    packed = state.astype(jnp.bfloat16)
    for k in range(8):
        packed_ref[32:, k * 128 : (k + 1) * 128] = packed[k * 16 : (k + 1) * 16]
    high, low = halves(jnp.broadcast_to(ended, (16, HD)))
    packed_ref[32:, 1024:1152] = high
    packed_ref[32:, 1152:1280] = low
    packed_ref[32:, 1280:] = jnp.zeros((16, 256), jnp.bfloat16)
    for k in range(5):
        packed_ref[:32, k * 256 : k * 256 + 128] = gate_ref[:, k * 128 : (k + 1) * 128]
        packed_ref[:32, k * 256 + 128 : (k + 1) * 256] = up_ref[:, k * 128 : (k + 1) * 128]
    packed_ref[:32, 1280:1408] = jnp.concatenate([gate_ref[:, 640:], up_ref[:, 640:]], axis=1)
    packed_ref[:32, 1408:] = jnp.concatenate(
        [turned_ref[:, 640:], jnp.zeros((32, 64), jnp.bfloat16)], axis=1
    )


def scanned(*operands):
    return pl.pallas_call(
        scan_kernel,
        out_shape=(
            jax.ShapeDtypeStruct((256, HD), jnp.float32),
            jax.ShapeDtypeStruct((256, HD), jnp.bfloat16),
            jax.ShapeDtypeStruct((48, 1536), jnp.bfloat16),
        ),
        in_specs=[whole()] * 8,
        out_specs=(whole(),) * 3,
        cost_estimate=pl.CostEstimate(
            flops=4_000_000_000, bytes_accessed=500_000, transcendentals=300_000
        ),
        name="scan",
    )(*operands)


def y_kernel(y_ref, pieces_ref, turned_ref, total_ref, here_ref):
    y = y_ref[0]
    total_sum = here_sum = jnp.zeros((1, HD), jnp.float32)
    total = here = jnp.zeros((HD, HD), jnp.float32)
    for k in range(4):
        here = jnp.where(k == y, total, here)
        here_sum = jnp.where(k == y, total_sum, here_sum)
        state = jnp.concatenate(
            [pieces_ref[k, 32:, j * 128 : (j + 1) * 128] for j in range(8)], axis=0
        ).astype(jnp.float32)
        one = pieces_ref[k, 32:, 1024:1152].astype(jnp.float32)[:1]
        one = one + pieces_ref[k, 32:, 1152:1280].astype(jnp.float32)[:1]
        total = jnp.exp(one) * total + state
        total_sum = total_sum + one
    here_ref[:HD, :] = here
    here_ref[HD:, :] = jnp.broadcast_to(here_sum, (8, HD))
    total_ref[:32, :] = turned_ref[:, :640].astype(jnp.float32) * SCALE
    for k in range(4):
        total_ref[32:, k * 128 : (k + 1) * 128] = total[k * 32 : (k + 1) * 32] * STATE_SCALE
    total_ref[32:, 512:] = jnp.broadcast_to(total_sum, (32, HD))


def joined_over_y(y, pieces, turned):
    return pl.pallas_call(
        y_kernel,
        out_shape=(
            jax.ShapeDtypeStruct((64, 640), jnp.float32),
            jax.ShapeDtypeStruct((136, HD), jnp.float32),
        ),
        in_specs=[whole(pltpu.SMEM), whole(), whole()],
        out_specs=(whole(), whole()),
        cost_estimate=pl.CostEstimate(
            flops=1_000_000_000, bytes_accessed=700_000, transcendentals=1000
        ),
        name="join",
    )(y, pieces, turned)


def mix_kernel(z_ref, lines_ref, here_ref, out_ref, scaled_ref, logits_ref, gain_ref, gated_ref):
    z = z_ref[0]
    before = jnp.zeros((HD, HD), jnp.float32)
    for k in range(15):
        state = jnp.concatenate(
            [lines_ref[k, :, j * 128 : (j + 1) * 128] for j in range(4)], axis=0
        )
        joined = jnp.exp(lines_ref[k, :1, 512:]) * before + state
        before = jnp.where(k < z, joined, before)
    here = here_ref[...]
    state = jnp.exp(here[HD : HD + 1]) * (before * (1.0 / STATE_SCALE)) + here[:HD]
    mixed = out_ref[...] + dot(scaled_ref[...], state, NT)
    normed = mixed * lax.rsqrt(jnp.mean(mixed * mixed, axis=-1, keepdims=True) + eps)
    logits = logits_ref[...].astype(jnp.float32)
    gated_ref[...] = (normed * gain_ref[...] * (logits * jax.nn.sigmoid(logits))).astype(
        jnp.bfloat16
    )


def mixed_rows(z, lines, here, out, scaled, logits, gain):
    return pl.pallas_call(
        mix_kernel,
        out_shape=jax.ShapeDtypeStruct((256, HD), jnp.bfloat16),
        in_specs=[whole(pltpu.SMEM)] + [whole()] * 6,
        out_specs=whole(),
        cost_estimate=pl.CostEstimate(
            flops=2_000_000_000, bytes_accessed=2_000_000, transcendentals=100_000
        ),
        name="mix",
    )(z, lines, here, out, scaled, logits, gain)


def ffn_kernel(
    place_ref,
    rows_ref,
    wide_ref,
    own_ref,
    down1_ref,
    up1_ref,
    far_ref,
    mine_ref,
    theirs_ref,
    columns,
    rest,
    weights,
    hidden,
    column_sems,
    piece_sems,
):
    y, core = place_ref[0], place_ref[1]
    places = [lax.rem(y + k, 4) for k in range(4)]
    column_copies = [
        pltpu.make_async_copy(
            wide_ref.at[:, pl.ds(n * 256, 256)], columns.at[n], column_sems.at[n]
        )
        for n in range(5)
    ]
    rest_copy = pltpu.make_async_copy(wide_ref.at[:, pl.ds(1280, 256)], rest, column_sems.at[5])
    piece_copies = [
        pltpu.make_async_copy(ref, weights.at[:, places[k]], piece_sems.at[n])
        for n, (ref, k) in enumerate(
            (
                (own_ref, 0),
                (up1_ref, 1),
                (far_ref, 2),
                (down1_ref, 3),
            )
        )
    ]
    for copy in column_copies:
        copy.start()
    rest_copy.start()
    for copy in piece_copies:
        copy.start()
    rows = rows_ref[...]

    for n in range(5):
        column_copies[n].wait()
        both = jnp.dot(rows, columns[n], preferred_element_type=jnp.float32)
        gate, up = both[:, :128], both[:, 128:]
        hidden[:, n * 128 : (n + 1) * 128] = (gate * jax.nn.sigmoid(gate) * up).astype(
            jnp.bfloat16
        )
    rest_copy.wait()
    both = jnp.dot(rows, rest[:, :128], preferred_element_type=jnp.float32)
    gate, up = both[:, :64], both[:, 64:]
    hidden[:, 640:704] = (gate * jax.nn.sigmoid(gate) * up).astype(jnp.bfloat16)
    for copy in piece_copies:
        copy.wait()
    first, second = hidden[:, :640], hidden[:, 640:704]

    @pl.loop(0, 8)
    def _(n):
        at = pl.multiple_of(n * 256, 256)
        part = lax.dot_general(
            first,
            weights[pl.ds(n * 2, 2)].reshape(256, 640),
            NT,
            preferred_element_type=jnp.float32,
        ) + lax.dot_general(
            second,
            rest[pl.ds(at, 256), 128:192],
            NT,
            preferred_element_type=jnp.float32,
        )
        part = part.astype(jnp.bfloat16).reshape(4, 2, 32, 256)
        mine_ref[:, :, pl.ds(at, 256)] = jnp.where(core == 0, part[:, 0], part[:, 1])
        theirs_ref[:, :, pl.ds(at, 256)] = jnp.where(core == 0, part[:, 1], part[:, 0])


def ffn(place, rows, wide, *pieces):
    pieces = [piece.reshape(16, 32, 640) for piece in pieces]
    half = jax.ShapeDtypeStruct((4, 32, 2048), jnp.bfloat16)
    return pl.pallas_call(
        ffn_kernel,
        out_shape=(half, half),
        in_specs=[whole(pltpu.SMEM), whole()] + [whole(pltpu.HBM)] * 5,
        out_specs=(whole(), whole()),
        scratch_shapes=[
            pltpu.VMEM((5, 2048, 256), jnp.bfloat16),
            pltpu.VMEM((2048, 256), jnp.bfloat16),
            pltpu.VMEM((16, 4, 32, 640), jnp.bfloat16),
            pltpu.VMEM((256, 768), jnp.bfloat16),
            pltpu.SemaphoreType.DMA((6,)),
            pltpu.SemaphoreType.DMA((4,)),
        ],
        compiler_params=pltpu.CompilerParams(vmem_limit_bytes=60 * 2**20),
        cost_estimate=pl.CostEstimate(
            flops=2 * 256 * 2048 * 2112, bytes_accessed=11 * 2**20, transcendentals=256 * 704
        ),
        name="ffn",
    )(place, rows, wide, *pieces)


def local(
    residual,
    queries,
    forget_gate_logits,
    projected_values,
    output_gate_logits,
    lower_bound_margin,
    extra_forget_logs,
    per_head_norm_gain,
    output_weight,
    feedforward_norm_gain,
    gate_weight,
    up_weight,
    down_weight,
):
    y = lax.axis_index("y").reshape(1)
    z = lax.axis_index("z").reshape(1)
    core = lax.axis_index("c")
    turned = down_weight.T
    out_rows, scaled, packed = scanned(
        queries,
        forget_gate_logits,
        projected_values,
        lower_bound_margin.reshape(1, HD),
        extra_forget_logs,
        gate_weight,
        up_weight,
        turned,
    )
    with jax.named_scope("ygather"):
        along_y = lax.all_gather(packed, "y")
    with jax.named_scope("widegather"):
        wide = lax.all_gather(along_y[:, :32].reshape(128, 1536), "z", axis=0, tiled=True)
    with jax.named_scope("outgather"):
        out_copies = jnp.broadcast_to(output_weight, (4, *output_weight.shape))
        out_mine = lax.all_to_all(out_copies, "x", split_axis=0, concat_axis=0, tiled=True)
    total, here = joined_over_y(y, along_y, turned)
    with jax.named_scope("zgather"):
        along_z = lax.all_gather(total.astype(jnp.float16), "z")
    own = (along_z[:, :32].astype(jnp.float32) * (1.0 / SCALE)).astype(jnp.bfloat16)
    own = own.reshape(512, 640)
    down1 = shifted(own, "y", 1)
    up1 = shifted(own, "y", -1)
    far = shifted(own, "y", 2)
    lines = along_z[:, 32:].astype(jnp.float32)
    lines, out_mine = lax.optimization_barrier((lines, out_mine))
    out_other = shifted(out_mine, "c", 1)
    gated = mixed_rows(
        z,
        lines,
        here,
        out_rows,
        scaled,
        output_gate_logits,
        per_head_norm_gain.reshape(1, HD),
    )
    with jax.named_scope("gatedgather"):
        gated_all = lax.all_gather(gated, TP)
    gated_all = gated_all.reshape(4, 2, 256, HD)
    projected = 0.0
    for which, weight in ((core, out_mine), (1 - core, out_other)):
        heads = lax.dynamic_index_in_dim(gated_all, which, 1, keepdims=False)
        projected = projected + jnp.dot(
            heads.transpose(1, 0, 2).reshape(256, 512),
            weight.reshape(512, 2048),
            preferred_element_type=jnp.float32,
        )
    after_mixer = (residual.astype(jnp.float32) + projected).astype(jnp.bfloat16)
    widened = after_mixer.astype(jnp.float32)
    normed = (
        widened
        * lax.rsqrt(jnp.mean(widened * widened, axis=-1, keepdims=True) + eps)
        * feedforward_norm_gain
    ).astype(jnp.bfloat16)
    places = jnp.stack([lax.axis_index("y"), core])
    mine, theirs = ffn(places, normed, wide, own, down1, up1, far)
    swapped = shifted(theirs, "c", 1)
    pair = (mine.astype(jnp.float32) + swapped.astype(jnp.float32)).astype(jnp.bfloat16)
    place = lax.axis_index(TP) * 32
    own_rows = lax.dynamic_slice_in_dim(after_mixer, place, 32, 0)
    pair, own_rows = lax.optimization_barrier((pair, own_rows))
    arrived = lax.all_to_all(pair, "x", split_axis=0, concat_axis=0, tiled=True)
    ffn_sum = arrived.astype(jnp.float32).sum(axis=0)
    finished = (own_rows.astype(jnp.float32) + 0.5 * ffn_sum).astype(jnp.bfloat16)
    along_x = lax.all_gather(finished, "x")
    others = shifted(along_x, "c", 1)
    first = jnp.where(core == 0, along_x, others)
    second = jnp.where(core == 0, others, along_x)
    return jnp.stack([first, second], axis=1).reshape(256, 2048)


def solution(mesh):
    finer = Mesh(mesh.devices.reshape(16, 4, 4, 2), ("z", "y", "x", "c"))
    placed = (
        P(SP, None),
        P(SP, TP),
        P(SP, TP),
        P(SP, TP),
        P(SP, TP),
        P(TP),
        P(SP, TP),
        P(),
        P(TP, None),
        P(),
        P(SP, TP),
        P(SP, TP),
        P(TP, SP),
    )
    return jax.shard_map(local, mesh=finer, in_specs=placed, out_specs=P(SP, None), check_vma=False)
```

```python
import jax
import jax.numpy as jnp
from jax import lax
from jax.experimental import pallas as pl
from jax.experimental.pallas import tpu as pltpu
from jax.sharding import Mesh
from jax.sharding import PartitionSpec as P


HD = 128
BLOCK = 64
SP = ("z", "y")
TP = ("x", "c")
SCALE = 2.0**18
STATE_SCALE = 2.0**10
NN = (((1,), (0,)), ((), ()))
NT = (((1,), (1,)), ((), ()))
TN = (((0,), (0,)), ((), ()))


eps = 1e-06


def shifted(value, axis, step):
    size = lax.axis_size(axis)
    return lax.ppermute(value, axis, [(k, (k + step) % size) for k in range(size)])


def whole(space=pltpu.VMEM):
    return pl.BlockSpec(memory_space=space)


def dot(left, right, dims=NN):
    return lax.dot_general(
        left.astype(jnp.bfloat16),
        right.astype(jnp.bfloat16),
        dims,
        preferred_element_type=jnp.float32,
    )


def halves(value):
    high = value.astype(jnp.bfloat16)
    return high, (value - high.astype(jnp.float32)).astype(jnp.bfloat16)


def scan_kernel(
    q_ref,
    f_ref,
    v_ref,
    margin_ref,
    extra_ref,
    gate_ref,
    up_ref,
    turned_ref,
    out_ref,
    scaled_ref,
    packed_ref,
):
    queries = q_ref[...].astype(jnp.float32)
    inflow = margin_ref[...] * jax.nn.sigmoid(-f_ref[...].astype(jnp.float32))
    keep_log = jnp.log1p(-inflow) + extra_ref[...]
    row = lax.broadcasted_iota(jnp.int32, (256, 256), 0)
    column = lax.broadcasted_iota(jnp.int32, (256, 256), 1)
    lower = (column <= row).astype(jnp.float32)
    total = jnp.dot(
        lower, keep_log, precision=lax.Precision.HIGHEST, preferred_element_type=jnp.float32
    )
    scaled_ref[...] = (queries * jnp.exp(total)).astype(jnp.bfloat16)
    causal = lax.broadcasted_iota(jnp.int32, (BLOCK, BLOCK), 1) <= lax.broadcasted_iota(
        jnp.int32, (BLOCK, BLOCK), 0
    )
    state = None
    ended = jnp.zeros((1, HD), jnp.float32)
    for k in range(256 // BLOCK):
        rows = slice(k * BLOCK, (k + 1) * BLOCK)
        inside, sums = queries[rows], total[rows]
        middle, end = sums[BLOCK // 2 - 1 : BLOCK // 2], sums[BLOCK - 1 :]
        values = v_ref[rows]
        scores = dot(inside * jnp.exp(sums - middle), inflow[rows] * jnp.exp(middle - sums), NT)
        result = dot(jnp.where(causal, scores, 0.0), values)
        added = dot(values, inflow[rows] * jnp.exp(end - sums), TN)
        if state is not None:
            result = result + dot(inside * jnp.exp(sums - ended), state, NT)
            added = added + jnp.exp(end - ended) * state
        out_ref[rows, :] = result
        state, ended = added, end
    packed = state.astype(jnp.bfloat16)
    for k in range(8):
        packed_ref[32:, k * 128 : (k + 1) * 128] = packed[k * 16 : (k + 1) * 16]
    high, low = halves(jnp.broadcast_to(ended, (16, HD)))
    packed_ref[32:, 1024:1152] = high
    packed_ref[32:, 1152:1280] = low
    packed_ref[32:, 1280:] = jnp.zeros((16, 256), jnp.bfloat16)
    for k in range(5):
        packed_ref[:32, k * 256 : k * 256 + 128] = gate_ref[:, k * 128 : (k + 1) * 128]
        packed_ref[:32, k * 256 + 128 : (k + 1) * 256] = up_ref[:, k * 128 : (k + 1) * 128]
    packed_ref[:32, 1280:1408] = jnp.concatenate([gate_ref[:, 640:], up_ref[:, 640:]], axis=1)
    packed_ref[:32, 1408:] = jnp.concatenate(
        [turned_ref[:, 640:], jnp.zeros((32, 64), jnp.bfloat16)], axis=1
    )


def scanned(*operands):
    return pl.pallas_call(
        scan_kernel,
        out_shape=(
            jax.ShapeDtypeStruct((256, HD), jnp.float32),
            jax.ShapeDtypeStruct((256, HD), jnp.bfloat16),
            jax.ShapeDtypeStruct((48, 1536), jnp.bfloat16),
        ),
        in_specs=[whole()] * 8,
        out_specs=(whole(),) * 3,
        cost_estimate=pl.CostEstimate(
            flops=4_000_000_000, bytes_accessed=500_000, transcendentals=300_000
        ),
        name="scan",
    )(*operands)


def y_kernel(y_ref, pieces_ref, turned_ref, total_ref, here_ref):
    y = y_ref[0]
    total_sum = here_sum = jnp.zeros((1, HD), jnp.float32)
    total = here = jnp.zeros((HD, HD), jnp.float32)
    for k in range(4):
        here = jnp.where(k == y, total, here)
        here_sum = jnp.where(k == y, total_sum, here_sum)
        state = jnp.concatenate(
            [pieces_ref[k, 32:, j * 128 : (j + 1) * 128] for j in range(8)], axis=0
        ).astype(jnp.float32)
        one = pieces_ref[k, 32:, 1024:1152].astype(jnp.float32)[:1]
        one = one + pieces_ref[k, 32:, 1152:1280].astype(jnp.float32)[:1]
        total = jnp.exp(one) * total + state
        total_sum = total_sum + one
    here_ref[:HD, :] = here
    here_ref[HD:, :] = jnp.broadcast_to(here_sum, (8, HD))
    total_ref[:32, :] = turned_ref[:, :640].astype(jnp.float32) * SCALE
    for k in range(4):
        total_ref[32:, k * 128 : (k + 1) * 128] = total[k * 32 : (k + 1) * 32] * STATE_SCALE
    total_ref[32:, 512:] = jnp.broadcast_to(total_sum, (32, HD))


def joined_over_y(y, pieces, turned):
    return pl.pallas_call(
        y_kernel,
        out_shape=(
            jax.ShapeDtypeStruct((64, 640), jnp.float32),
            jax.ShapeDtypeStruct((136, HD), jnp.float32),
        ),
        in_specs=[whole(pltpu.SMEM), whole(), whole()],
        out_specs=(whole(), whole()),
        cost_estimate=pl.CostEstimate(
            flops=1_000_000_000, bytes_accessed=700_000, transcendentals=1000
        ),
        name="join",
    )(y, pieces, turned)


def mix_kernel(z_ref, lines_ref, here_ref, out_ref, scaled_ref, logits_ref, gain_ref, gated_ref):
    z = z_ref[0]
    before = jnp.zeros((HD, HD), jnp.float32)
    for k in range(15):
        state = jnp.concatenate(
            [lines_ref[k, :, j * 128 : (j + 1) * 128] for j in range(4)], axis=0
        )
        joined = jnp.exp(lines_ref[k, :1, 512:]) * before + state
        before = jnp.where(k < z, joined, before)
    here = here_ref[...]
    state = jnp.exp(here[HD : HD + 1]) * (before * (1.0 / STATE_SCALE)) + here[:HD]
    mixed = out_ref[...] + dot(scaled_ref[...], state, NT)
    normed = mixed * lax.rsqrt(jnp.mean(mixed * mixed, axis=-1, keepdims=True) + eps)
    logits = logits_ref[...].astype(jnp.float32)
    gated_ref[...] = (normed * gain_ref[...] * (logits * jax.nn.sigmoid(logits))).astype(
        jnp.bfloat16
    )


def mixed_rows(z, lines, here, out, scaled, logits, gain):
    return pl.pallas_call(
        mix_kernel,
        out_shape=jax.ShapeDtypeStruct((256, HD), jnp.bfloat16),
        in_specs=[whole(pltpu.SMEM)] + [whole()] * 6,
        out_specs=whole(),
        cost_estimate=pl.CostEstimate(
            flops=2_000_000_000, bytes_accessed=2_000_000, transcendentals=100_000
        ),
        name="mix",
    )(z, lines, here, out, scaled, logits, gain)


def ffn_kernel(
    y_ref,
    core_ref,
    rows_ref,
    wide_ref,
    own_ref,
    down1_ref,
    up1_ref,
    far_ref,
    mine_ref,
    theirs_ref,
    bands,
    half,
    weights,
    hidden,
    band_sems,
    piece_sems,
):
    y, core = y_ref[0], core_ref[0]
    places = [lax.rem(y + k, 4) for k in range(4)]
    band_copies = [
        pltpu.make_async_copy(
            wide_ref.at[pl.ds(n * 1024, 1024)], bands.at[pl.ds(n * 1024, 1024)], band_sems.at[n]
        )
        for n in range(2)
    ]
    piece_copies = [
        pltpu.make_async_copy(ref, weights.at[:, places[k]], piece_sems.at[n])
        for n, (ref, k) in enumerate(
            (
                (own_ref, 0),
                (up1_ref, 1),
                (far_ref, 2),
                (down1_ref, 3),
            )
        )
    ]
    for copy in band_copies:
        copy.start()
    for copy in piece_copies:
        copy.start()
    spans = [slice(n * 256, min(n * 256 + 256, 1408)) for n in range(6)]
    rows = rows_ref[:, :1024]
    band_copies[0].wait()
    for span in spans:
        half[:, span] = jnp.dot(rows, bands[:1024, span], preferred_element_type=jnp.float32)
    rows = rows_ref[:, 1024:]
    band_copies[1].wait()
    for n, span in enumerate(spans):
        both = half[:, span] + jnp.dot(
            rows, bands[1024:, span], preferred_element_type=jnp.float32
        )
        width = both.shape[1] // 2
        gate, up = both[:, :width], both[:, width:]
        hidden[:, n * 128 : n * 128 + width] = (gate * jax.nn.sigmoid(gate) * up).astype(
            jnp.bfloat16
        )
    for copy in piece_copies:
        copy.wait()
    first, second = hidden[:, :640], hidden[:, 640:704]

    @pl.loop(0, 8)
    def _(n):
        at = pl.multiple_of(n * 256, 256)
        part = lax.dot_general(
            first,
            weights[pl.ds(n * 2, 2)].reshape(256, 640),
            NT,
            preferred_element_type=jnp.float32,
        ) + lax.dot_general(
            second,
            bands[pl.ds(at, 256), 1408:1472],
            NT,
            preferred_element_type=jnp.float32,
        )
        part = part.astype(jnp.bfloat16).reshape(4, 2, 32, 256)
        mine_ref[:, :, pl.ds(at, 256)] = jnp.where(core == 0, part[:, 0], part[:, 1])
        theirs_ref[:, :, pl.ds(at, 256)] = jnp.where(core == 0, part[:, 1], part[:, 0])


def ffn(y, core, rows, wide, *pieces):
    pieces = [piece.reshape(16, 32, 640) for piece in pieces]
    half = jax.ShapeDtypeStruct((4, 32, 2048), jnp.bfloat16)
    return pl.pallas_call(
        ffn_kernel,
        out_shape=(half, half),
        in_specs=[whole(pltpu.SMEM)] * 2 + [whole()] + [whole(pltpu.HBM)] * 5,
        out_specs=(whole(), whole()),
        scratch_shapes=[
            pltpu.VMEM((2048, 1536), jnp.bfloat16),
            pltpu.VMEM((256, 1408), jnp.float32),
            pltpu.VMEM((16, 4, 32, 640), jnp.bfloat16),
            pltpu.VMEM((256, 768), jnp.bfloat16),
            pltpu.SemaphoreType.DMA((2,)),
            pltpu.SemaphoreType.DMA((4,)),
        ],
        compiler_params=pltpu.CompilerParams(vmem_limit_bytes=60 * 2**20),
        cost_estimate=pl.CostEstimate(
            flops=2 * 256 * 2048 * 2112, bytes_accessed=11 * 2**20, transcendentals=256 * 704
        ),
        name="ffn",
    )(y, core, rows, wide, *pieces)


def local(
    residual,
    queries,
    forget_gate_logits,
    projected_values,
    output_gate_logits,
    lower_bound_margin,
    extra_forget_logs,
    per_head_norm_gain,
    output_weight,
    feedforward_norm_gain,
    gate_weight,
    up_weight,
    down_weight,
):
    y = lax.axis_index("y").reshape(1)
    z = lax.axis_index("z").reshape(1)
    core = lax.axis_index("c")
    turned = down_weight.T
    out_rows, scaled, packed = scanned(
        queries,
        forget_gate_logits,
        projected_values,
        lower_bound_margin.reshape(1, HD),
        extra_forget_logs,
        gate_weight,
        up_weight,
        turned,
    )
    along_y = lax.all_gather(packed, "y")
    wide = lax.all_gather(along_y[:, :32].reshape(128, 1536), "z", axis=0, tiled=True)
    out_copies = jnp.broadcast_to(output_weight, (4, *output_weight.shape))
    out_mine = lax.all_to_all(out_copies, "x", split_axis=0, concat_axis=0, tiled=True)
    total, here = joined_over_y(y, along_y, turned)
    along_z = lax.all_gather(total.astype(jnp.float16), "z")
    own = (along_z[:, :32].astype(jnp.float32) * (1.0 / SCALE)).astype(jnp.bfloat16)
    own = own.reshape(512, 640)
    down1 = shifted(own, "y", 1)
    up1 = shifted(own, "y", -1)
    far = shifted(own, "y", 2)
    lines = along_z[:, 32:].astype(jnp.float32)
    lines, out_mine, own = lax.optimization_barrier((lines, out_mine, own))
    out_other = shifted(out_mine, "c", 1)
    gated = mixed_rows(
        z,
        lines,
        here,
        out_rows,
        scaled,
        output_gate_logits,
        per_head_norm_gain.reshape(1, HD),
    )
    heads = lax.all_to_all(
        jnp.broadcast_to(gated, (4, 256, HD)), "x", split_axis=0, concat_axis=0, tiled=True
    )
    heads_other = shifted(heads, "c", 1)
    projected = 0.0
    for part, weight in ((heads, out_mine), (heads_other, out_other)):
        projected = projected + jnp.dot(
            part.transpose(1, 0, 2).reshape(256, 512),
            weight.reshape(512, 2048),
            preferred_element_type=jnp.float32,
        )
    after_mixer = (residual.astype(jnp.float32) + projected).astype(jnp.bfloat16)
    widened = after_mixer.astype(jnp.float32)
    normed = (
        widened
        * lax.rsqrt(jnp.mean(widened * widened, axis=-1, keepdims=True) + eps)
        * feedforward_norm_gain
    ).astype(jnp.bfloat16)
    mine, theirs = ffn(y, core.reshape(1), normed, wide, own, down1, up1, far)
    swapped = shifted(theirs, "c", 1)
    pair = (mine.astype(jnp.float32) + swapped.astype(jnp.float32)).astype(jnp.bfloat16)
    place = lax.axis_index(TP) * 32
    own_rows = lax.dynamic_slice_in_dim(after_mixer, place, 32, 0)
    pair, own_rows = lax.optimization_barrier((pair, own_rows))
    arrived = lax.all_to_all(pair, "x", split_axis=0, concat_axis=0, tiled=True)
    ffn_sum = arrived.astype(jnp.float32).sum(axis=0)
    finished = (own_rows.astype(jnp.float32) + 0.5 * ffn_sum).astype(jnp.bfloat16)
    along_x = lax.all_gather(finished, "x")
    others = shifted(along_x, "c", 1)
    first = jnp.where(core == 0, along_x, others)
    second = jnp.where(core == 0, others, along_x)
    return jnp.stack([first, second], axis=1).reshape(256, 2048)


def solution(mesh):
    finer = Mesh(mesh.devices.reshape(16, 4, 4, 2), ("z", "y", "x", "c"))
    placed = (
        P(SP, None),
        P(SP, TP),
        P(SP, TP),
        P(SP, TP),
        P(SP, TP),
        P(TP),
        P(SP, TP),
        P(),
        P(TP, None),
        P(),
        P(SP, TP),
        P(SP, TP),
        P(TP, SP),
    )
    return jax.shard_map(
        local, mesh=finer, in_specs=placed, out_specs=P(SP, None), check_vma=False
    )
```

```python
import jax
import jax.numpy as jnp
from jax import lax
from jax.experimental import pallas as pl
from jax.experimental.pallas import tpu as pltpu
from jax.sharding import Mesh
from jax.sharding import PartitionSpec as P


HD = 128
BLOCK = 64
SP = ("z", "y")
TP = ("x", "c")
SCALE = 2.0**18
STATE_SCALE = 2.0**10
NN = (((1,), (0,)), ((), ()))
NT = (((1,), (1,)), ((), ()))
TN = (((0,), (0,)), ((), ()))


eps = 1e-06


def shifted(value, axis, step):
    size = lax.axis_size(axis)
    return lax.ppermute(value, axis, [(k, (k + step) % size) for k in range(size)])


def whole(space=pltpu.VMEM):
    return pl.BlockSpec(memory_space=space)


def dot(left, right, dims=NN):
    return lax.dot_general(
        left.astype(jnp.bfloat16),
        right.astype(jnp.bfloat16),
        dims,
        preferred_element_type=jnp.float32,
    )


def halves(value):
    high = value.astype(jnp.bfloat16)
    return high, (value - high.astype(jnp.float32)).astype(jnp.bfloat16)


def scan_kernel(
    q_ref,
    f_ref,
    v_ref,
    margin_ref,
    extra_ref,
    gate_ref,
    up_ref,
    turned_ref,
    out_ref,
    scaled_ref,
    packed_ref,
):
    queries = q_ref[...].astype(jnp.float32)
    inflow = margin_ref[...] * jax.nn.sigmoid(-f_ref[...].astype(jnp.float32))
    keep_log = jnp.log1p(-inflow) + extra_ref[...]
    row = lax.broadcasted_iota(jnp.int32, (256, 256), 0)
    column = lax.broadcasted_iota(jnp.int32, (256, 256), 1)
    lower = (column <= row).astype(jnp.float32)
    total = jnp.dot(
        lower, keep_log, precision=lax.Precision.HIGHEST, preferred_element_type=jnp.float32
    )
    scaled_ref[...] = (queries * jnp.exp(total)).astype(jnp.bfloat16)
    causal = lax.broadcasted_iota(jnp.int32, (BLOCK, BLOCK), 1) <= lax.broadcasted_iota(
        jnp.int32, (BLOCK, BLOCK), 0
    )
    state = None
    ended = jnp.zeros((1, HD), jnp.float32)
    for k in range(256 // BLOCK):
        rows = slice(k * BLOCK, (k + 1) * BLOCK)
        inside, sums = queries[rows], total[rows]
        middle, end = sums[BLOCK // 2 - 1 : BLOCK // 2], sums[BLOCK - 1 :]
        values = v_ref[rows]
        scores = dot(inside * jnp.exp(sums - middle), inflow[rows] * jnp.exp(middle - sums), NT)
        result = dot(jnp.where(causal, scores, 0.0), values)
        added = dot(values, inflow[rows] * jnp.exp(end - sums), TN)
        if state is not None:
            result = result + dot(inside * jnp.exp(sums - ended), state, NT)
            added = added + jnp.exp(end - ended) * state
        out_ref[rows, :] = result
        state, ended = added, end
    packed = state.astype(jnp.bfloat16)
    for k in range(8):
        packed_ref[32:, k * 128 : (k + 1) * 128] = packed[k * 16 : (k + 1) * 16]
    high, low = halves(jnp.broadcast_to(ended, (16, HD)))
    packed_ref[32:, 1024:1152] = high
    packed_ref[32:, 1152:1280] = low
    packed_ref[32:, 1280:] = jnp.zeros((16, 256), jnp.bfloat16)
    for k in range(5):
        packed_ref[:32, k * 256 : k * 256 + 128] = gate_ref[:, k * 128 : (k + 1) * 128]
        packed_ref[:32, k * 256 + 128 : (k + 1) * 256] = up_ref[:, k * 128 : (k + 1) * 128]
    packed_ref[:32, 1280:1408] = jnp.concatenate([gate_ref[:, 640:], up_ref[:, 640:]], axis=1)
    packed_ref[:32, 1408:] = jnp.concatenate(
        [turned_ref[:, 640:], jnp.zeros((32, 64), jnp.bfloat16)], axis=1
    )


def scanned(*operands):
    return pl.pallas_call(
        scan_kernel,
        out_shape=(
            jax.ShapeDtypeStruct((256, HD), jnp.float32),
            jax.ShapeDtypeStruct((256, HD), jnp.bfloat16),
            jax.ShapeDtypeStruct((48, 1536), jnp.bfloat16),
        ),
        in_specs=[whole()] * 8,
        out_specs=(whole(),) * 3,
        cost_estimate=pl.CostEstimate(
            flops=4_000_000_000, bytes_accessed=500_000, transcendentals=300_000
        ),
        name="scan",
    )(*operands)


def y_kernel(y_ref, pieces_ref, turned_ref, total_ref, here_ref):
    y = y_ref[0]
    total_sum = here_sum = jnp.zeros((1, HD), jnp.float32)
    total = here = jnp.zeros((HD, HD), jnp.float32)
    for k in range(4):
        here = jnp.where(k == y, total, here)
        here_sum = jnp.where(k == y, total_sum, here_sum)
        state = jnp.concatenate(
            [pieces_ref[k, 32:, j * 128 : (j + 1) * 128] for j in range(8)], axis=0
        ).astype(jnp.float32)
        one = pieces_ref[k, 32:, 1024:1152].astype(jnp.float32)[:1]
        one = one + pieces_ref[k, 32:, 1152:1280].astype(jnp.float32)[:1]
        total = jnp.exp(one) * total + state
        total_sum = total_sum + one
    here_ref[:HD, :] = here
    here_ref[HD:, :] = jnp.broadcast_to(here_sum, (8, HD))
    total_ref[:32, :] = turned_ref[:, :640].astype(jnp.float32) * SCALE
    for k in range(4):
        total_ref[32:, k * 128 : (k + 1) * 128] = total[k * 32 : (k + 1) * 32] * STATE_SCALE
    total_ref[32:, 512:] = jnp.broadcast_to(total_sum, (32, HD))


def joined_over_y(y, pieces, turned):
    return pl.pallas_call(
        y_kernel,
        out_shape=(
            jax.ShapeDtypeStruct((64, 640), jnp.float32),
            jax.ShapeDtypeStruct((136, HD), jnp.float32),
        ),
        in_specs=[whole(pltpu.SMEM), whole(), whole()],
        out_specs=(whole(), whole()),
        cost_estimate=pl.CostEstimate(
            flops=1_000_000_000, bytes_accessed=700_000, transcendentals=1000
        ),
        name="join",
    )(y, pieces, turned)


def mix_kernel(z_ref, lines_ref, here_ref, out_ref, scaled_ref, logits_ref, gain_ref, gated_ref):
    z = z_ref[0]
    before = jnp.zeros((HD, HD), jnp.float32)
    for k in range(15):
        state = jnp.concatenate(
            [lines_ref[k, :, j * 128 : (j + 1) * 128] for j in range(4)], axis=0
        )
        joined = jnp.exp(lines_ref[k, :1, 512:]) * before + state
        before = jnp.where(k < z, joined, before)
    here = here_ref[...]
    state = jnp.exp(here[HD : HD + 1]) * (before * (1.0 / STATE_SCALE)) + here[:HD]
    mixed = out_ref[...] + dot(scaled_ref[...], state, NT)
    normed = mixed * lax.rsqrt(jnp.mean(mixed * mixed, axis=-1, keepdims=True) + eps)
    logits = logits_ref[...].astype(jnp.float32)
    gated = (normed * gain_ref[...] * (logits * jax.nn.sigmoid(logits))).astype(jnp.bfloat16)
    gated_ref[...] = gated


def mixed_rows(z, lines, here, out, scaled, logits, gain):
    return pl.pallas_call(
        mix_kernel,
        out_shape=jax.ShapeDtypeStruct((256, HD), jnp.bfloat16),
        in_specs=[whole(pltpu.SMEM)] + [whole()] * 6,
        out_specs=whole(),
        cost_estimate=pl.CostEstimate(
            flops=2_000_000_000, bytes_accessed=2_000_000, transcendentals=100_000
        ),
        name="mix",
    )(z, lines, here, out, scaled, logits, gain)


def ffn_kernel(
    core_ref,
    after_ref,
    gain_ref,
    bands,
    pieces_ref,
    mine_ref,
    theirs_ref,
    normed,
    hidden,
):
    core = core_ref[0]
    for k in range(8):
        lines = slice(k * 32, (k + 1) * 32)
        after = after_ref[lines].astype(jnp.float32)
        scale = lax.rsqrt(jnp.mean(after * after, axis=-1, keepdims=True) + eps)
        normed[lines] = (after * scale * gain_ref[...]).astype(jnp.bfloat16)
    spans = [slice(n * 256, min(n * 256 + 256, 1408)) for n in range(6)]
    rows = normed[...]
    for n, span in enumerate(spans):
        both = jnp.dot(rows, bands[:, span], preferred_element_type=jnp.float32)
        width = both.shape[1] // 2
        gate, up = both[:, :width], both[:, width:]
        hidden[:, n * 128 : n * 128 + width] = (gate * jax.nn.sigmoid(gate) * up).astype(
            jnp.bfloat16
        )
    first, second = hidden[:, :640], hidden[:, 640:704]

    @pl.loop(0, 8)
    def _(n):
        at = pl.multiple_of(n * 256, 256)
        part = lax.dot_general(
            first,
            jnp.concatenate(
                [pieces_ref[k, n * 2 + j] for j in range(2) for k in range(4)], axis=0
            ),
            NT,
            preferred_element_type=jnp.float32,
        ) + lax.dot_general(
            second,
            bands[pl.ds(at, 256), 1408:1472],
            NT,
            preferred_element_type=jnp.float32,
        )
        part = part.astype(jnp.bfloat16).reshape(4, 2, 32, 256)
        mine_ref[:, :, pl.ds(at, 256)] = jnp.where(core == 0, part[:, 0], part[:, 1])
        theirs_ref[:, :, pl.ds(at, 256)] = jnp.where(core == 0, part[:, 1], part[:, 0])


def ffn(core, after, gain, wide, pieces):
    half = jax.ShapeDtypeStruct((4, 32, 2048), jnp.bfloat16)
    return pl.pallas_call(
        ffn_kernel,
        out_shape=(half, half),
        in_specs=[whole(pltpu.SMEM), whole(), whole(), whole(), whole()],
        out_specs=(whole(), whole()),
        scratch_shapes=[
            pltpu.VMEM((256, 2048), jnp.bfloat16),
            pltpu.VMEM((256, 768), jnp.bfloat16),
        ],
        compiler_params=pltpu.CompilerParams(vmem_limit_bytes=40 * 2**20),
        cost_estimate=pl.CostEstimate(
            flops=2 * 256 * 2048 * 2112, bytes_accessed=11 * 2**20, transcendentals=256 * 704
        ),
        name="ffn",
    )(core, after, gain, wide, pieces)


def local(
    residual,
    queries,
    forget_gate_logits,
    projected_values,
    output_gate_logits,
    lower_bound_margin,
    extra_forget_logs,
    per_head_norm_gain,
    output_weight,
    feedforward_norm_gain,
    gate_weight,
    up_weight,
    down_weight,
):
    y = lax.axis_index("y").reshape(1)
    z = lax.axis_index("z").reshape(1)
    core = lax.axis_index("c")
    turned = down_weight.T
    out_rows, scaled, packed = scanned(
        queries,
        forget_gate_logits,
        projected_values,
        lower_bound_margin.reshape(1, HD),
        extra_forget_logs,
        gate_weight,
        up_weight,
        turned,
    )
    along_y = lax.all_gather(packed, "y")
    wide = lax.all_gather(along_y[:, :32].reshape(128, 1536), "z", axis=0, tiled=True)
    out_copies = jnp.broadcast_to(output_weight, (4, *output_weight.shape))
    out_mine = lax.all_to_all(out_copies, "x", split_axis=0, concat_axis=0, tiled=True)
    total, here = joined_over_y(y, along_y, turned)
    along_z = lax.all_gather(total.astype(jnp.float16), "z")
    own = (along_z[:, :32].astype(jnp.float32) * (1.0 / SCALE)).astype(jnp.bfloat16)
    own = jnp.broadcast_to(own, (4, 16, 32, 640))
    pieces = lax.all_to_all(own, "y", split_axis=0, concat_axis=0, tiled=True)
    lines = along_z[:, 32:].astype(jnp.float32)
    lines, out_mine = lax.optimization_barrier((lines, out_mine))
    out_other = shifted(out_mine, "c", 1)
    gated = mixed_rows(
        z,
        lines,
        here,
        out_rows,
        scaled,
        output_gate_logits,
        per_head_norm_gain.reshape(1, HD),
    )
    heads = lax.all_gather(gated, "x")
    heads_other = shifted(heads, "c", 1)
    projected = 0.0
    for part, weight in ((heads, out_mine), (heads_other, out_other)):
        projected = projected + jnp.dot(
            part.transpose(1, 0, 2).reshape(256, 512),
            weight.reshape(512, 2048),
            preferred_element_type=jnp.float32,
        )
    after_mixer = (residual.astype(jnp.float32) + projected).astype(jnp.bfloat16)
    gain = feedforward_norm_gain.reshape(1, 2048)
    mine, theirs = ffn(core.reshape(1), after_mixer, gain, wide, pieces)
    swapped = shifted(theirs, "c", 1)
    pair = (mine.astype(jnp.float32) + swapped.astype(jnp.float32)).astype(jnp.bfloat16)
    place = lax.axis_index(TP) * 32
    own_rows = lax.dynamic_slice_in_dim(after_mixer, place, 32, 0)
    pair, own_rows = lax.optimization_barrier((pair, own_rows))
    arrived = lax.all_to_all(pair, "x", split_axis=0, concat_axis=0, tiled=True)
    ffn_sum = arrived.astype(jnp.float32).sum(axis=0)
    finished = (own_rows.astype(jnp.float32) + 0.5 * ffn_sum).astype(jnp.bfloat16)
    along_x = lax.all_gather(finished, "x")
    others = shifted(along_x, "c", 1)
    first = jnp.where(core == 0, along_x, others)
    second = jnp.where(core == 0, others, along_x)
    return jnp.stack([first, second], axis=1).reshape(256, 2048)


def solution(mesh):
    finer = Mesh(mesh.devices.reshape(16, 4, 4, 2), ("z", "y", "x", "c"))
    placed = (
        P(SP, None),
        P(SP, TP),
        P(SP, TP),
        P(SP, TP),
        P(SP, TP),
        P(TP),
        P(SP, TP),
        P(),
        P(TP, None),
        P(),
        P(SP, TP),
        P(SP, TP),
        P(TP, SP),
    )
    return jax.shard_map(
        local, mesh=finer, in_specs=placed, out_specs=P(SP, None), check_vma=False
    )
```

```python
import jax
import jax.numpy as jnp
from jax import lax
from jax.experimental import pallas as pl
from jax.experimental.pallas import tpu as pltpu
from jax.sharding import Mesh
from jax.sharding import PartitionSpec as P


HD = 128
BLOCK = 64
SP = ("z", "y")
TP = ("x", "c")
SCALE = 2.0**18
STATE_SCALE = 2.0**10
NN = (((1,), (0,)), ((), ()))
NT = (((1,), (1,)), ((), ()))
TN = (((0,), (0,)), ((), ()))


eps = 1e-06


def shifted(value, axis, step):
    size = lax.axis_size(axis)
    return lax.ppermute(value, axis, [(k, (k + step) % size) for k in range(size)])


def whole(space=pltpu.VMEM):
    return pl.BlockSpec(memory_space=space)


def dot(left, right, dims=NN):
    return lax.dot_general(
        left.astype(jnp.bfloat16),
        right.astype(jnp.bfloat16),
        dims,
        preferred_element_type=jnp.float32,
    )


def halves(value):
    high = value.astype(jnp.bfloat16)
    return high, (value - high.astype(jnp.float32)).astype(jnp.bfloat16)


def scan_kernel(
    q_ref,
    f_ref,
    v_ref,
    margin_ref,
    extra_ref,
    gate_ref,
    up_ref,
    turned_ref,
    out_ref,
    scaled_ref,
    packed_ref,
):
    queries = q_ref[...].astype(jnp.float32)
    inflow = margin_ref[...] * jax.nn.sigmoid(-f_ref[...].astype(jnp.float32))
    keep_log = jnp.log1p(-inflow) + extra_ref[...]
    row = lax.broadcasted_iota(jnp.int32, (256, 256), 0)
    column = lax.broadcasted_iota(jnp.int32, (256, 256), 1)
    lower = (column <= row).astype(jnp.float32)
    total = jnp.dot(
        lower, keep_log, precision=lax.Precision.HIGHEST, preferred_element_type=jnp.float32
    )
    scaled_ref[...] = (queries * jnp.exp(total)).astype(jnp.bfloat16)
    causal = lax.broadcasted_iota(jnp.int32, (BLOCK, BLOCK), 1) <= lax.broadcasted_iota(
        jnp.int32, (BLOCK, BLOCK), 0
    )
    state = None
    ended = jnp.zeros((1, HD), jnp.float32)
    for k in range(256 // BLOCK):
        rows = slice(k * BLOCK, (k + 1) * BLOCK)
        inside, sums = queries[rows], total[rows]
        middle, end = sums[BLOCK // 2 - 1 : BLOCK // 2], sums[BLOCK - 1 :]
        values = v_ref[rows]
        scores = dot(inside * jnp.exp(sums - middle), inflow[rows] * jnp.exp(middle - sums), NT)
        result = dot(jnp.where(causal, scores, 0.0), values)
        added = dot(values, inflow[rows] * jnp.exp(end - sums), TN)
        if state is not None:
            result = result + dot(inside * jnp.exp(sums - ended), state, NT)
            added = added + jnp.exp(end - ended) * state
        out_ref[rows, :] = result
        state, ended = added, end
    packed = state.astype(jnp.bfloat16)
    for k in range(8):
        packed_ref[32:, k * 128 : (k + 1) * 128] = packed[k * 16 : (k + 1) * 16]
    high, low = halves(jnp.broadcast_to(ended, (16, HD)))
    packed_ref[32:, 1024:1152] = high
    packed_ref[32:, 1152:1280] = low
    packed_ref[32:, 1280:] = jnp.zeros((16, 256), jnp.bfloat16)
    for k in range(5):
        packed_ref[:32, k * 256 : k * 256 + 128] = gate_ref[:, k * 128 : (k + 1) * 128]
        packed_ref[:32, k * 256 + 128 : (k + 1) * 256] = up_ref[:, k * 128 : (k + 1) * 128]
    packed_ref[:32, 1280:1408] = jnp.concatenate([gate_ref[:, 640:], up_ref[:, 640:]], axis=1)
    packed_ref[:32, 1408:] = jnp.concatenate(
        [turned_ref[:, 640:], jnp.zeros((32, 64), jnp.bfloat16)], axis=1
    )


def scanned(*operands):
    return pl.pallas_call(
        scan_kernel,
        out_shape=(
            jax.ShapeDtypeStruct((256, HD), jnp.float32),
            jax.ShapeDtypeStruct((256, HD), jnp.bfloat16),
            jax.ShapeDtypeStruct((48, 1536), jnp.bfloat16),
        ),
        in_specs=[whole()] * 8,
        out_specs=(whole(),) * 3,
        cost_estimate=pl.CostEstimate(
            flops=4_000_000_000, bytes_accessed=500_000, transcendentals=300_000
        ),
        name="scan",
    )(*operands)


def y_kernel(y_ref, pieces_ref, turned_ref, total_ref, here_ref):
    y = y_ref[0]
    total_sum = here_sum = jnp.zeros((1, HD), jnp.float32)
    total = here = jnp.zeros((HD, HD), jnp.float32)
    for k in range(4):
        here = jnp.where(k == y, total, here)
        here_sum = jnp.where(k == y, total_sum, here_sum)
        state = jnp.concatenate(
            [pieces_ref[k, 32:, j * 128 : (j + 1) * 128] for j in range(8)], axis=0
        ).astype(jnp.float32)
        one = pieces_ref[k, 32:, 1024:1152].astype(jnp.float32)[:1]
        one = one + pieces_ref[k, 32:, 1152:1280].astype(jnp.float32)[:1]
        total = jnp.exp(one) * total + state
        total_sum = total_sum + one
    here_ref[:HD, :] = here
    here_ref[HD:, :] = jnp.broadcast_to(here_sum, (8, HD))
    total_ref[:32, :] = turned_ref[:, :640].astype(jnp.float32) * SCALE
    for k in range(4):
        total_ref[32:, k * 128 : (k + 1) * 128] = total[k * 32 : (k + 1) * 32] * STATE_SCALE
    total_ref[32:, 512:] = jnp.broadcast_to(total_sum, (32, HD))


def joined_over_y(y, pieces, turned):
    return pl.pallas_call(
        y_kernel,
        out_shape=(
            jax.ShapeDtypeStruct((64, 640), jnp.float32),
            jax.ShapeDtypeStruct((136, HD), jnp.float32),
        ),
        in_specs=[whole(pltpu.SMEM), whole(), whole()],
        out_specs=(whole(), whole()),
        cost_estimate=pl.CostEstimate(
            flops=1_000_000_000, bytes_accessed=700_000, transcendentals=1000
        ),
        name="join",
    )(y, pieces, turned)


def mix_kernel(z_ref, lines_ref, here_ref, out_ref, scaled_ref, logits_ref, gain_ref, gated_ref):
    z = z_ref[0]
    before = jnp.zeros((HD, HD), jnp.float32)
    for k in range(15):
        state = jnp.concatenate(
            [lines_ref[k, :, j * 128 : (j + 1) * 128] for j in range(4)], axis=0
        )
        joined = jnp.exp(lines_ref[k, :1, 512:]) * before + state
        before = jnp.where(k < z, joined, before)
    here = here_ref[...]
    state = jnp.exp(here[HD : HD + 1]) * (before * (1.0 / STATE_SCALE)) + here[:HD]
    mixed = out_ref[...] + dot(scaled_ref[...], state, NT)
    normed = mixed * lax.rsqrt(jnp.mean(mixed * mixed, axis=-1, keepdims=True) + eps)
    logits = logits_ref[...].astype(jnp.float32)
    gated = (normed * gain_ref[...] * (logits * jax.nn.sigmoid(logits))).astype(jnp.bfloat16)
    gated_ref[...] = gated


def mixed_rows(z, lines, here, out, scaled, logits, gain):
    return pl.pallas_call(
        mix_kernel,
        out_shape=jax.ShapeDtypeStruct((256, HD), jnp.bfloat16),
        in_specs=[whole(pltpu.SMEM)] + [whole()] * 6,
        out_specs=whole(),
        cost_estimate=pl.CostEstimate(
            flops=2_000_000_000, bytes_accessed=2_000_000, transcendentals=100_000
        ),
        name="mix",
    )(z, lines, here, out, scaled, logits, gain)


def ffn_kernel(
    core_ref,
    after_ref,
    gain_ref,
    wide_ref,
    pieces_ref,
    mine_ref,
    theirs_ref,
    bands,
    after_rows,
    pieces,
    normed,
    half,
    hidden,
    band_sems,
):
    core = core_ref[0]
    band_copies = [
        pltpu.make_async_copy(
            wide_ref.at[pl.ds(start, size)], bands.at[pl.ds(start, size)], band_sems.at[n]
        )
        for n, (start, size) in enumerate(((0, 512), (512, 1536)))
    ]
    after_copy = pltpu.make_async_copy(after_ref, after_rows, band_sems.at[2])
    piece_copy = pltpu.make_async_copy(pieces_ref, pieces, band_sems.at[3])
    after_copy.start()
    for copy in band_copies:
        copy.start()
    piece_copy.start()
    after_copy.wait()
    for k in range(8):
        lines = slice(k * 32, (k + 1) * 32)
        after = after_rows[lines].astype(jnp.float32)
        scale = lax.rsqrt(jnp.mean(after * after, axis=-1, keepdims=True) + eps)
        normed[lines] = (after * scale * gain_ref[...]).astype(jnp.bfloat16)
    spans = [slice(n * 256, min(n * 256 + 256, 1408)) for n in range(6)]
    rows = normed[:, :512]
    band_copies[0].wait()
    for span in spans:
        half[:, span] = jnp.dot(rows, bands[:512, span], preferred_element_type=jnp.float32)
    rows = normed[:, 512:]
    band_copies[1].wait()
    for n, span in enumerate(spans):
        both = half[:, span] + jnp.dot(
            rows, bands[512:, span], preferred_element_type=jnp.float32
        )
        width = both.shape[1] // 2
        gate, up = both[:, :width], both[:, width:]
        hidden[:, n * 128 : n * 128 + width] = (gate * jax.nn.sigmoid(gate) * up).astype(
            jnp.bfloat16
        )
    piece_copy.wait()
    first, second = hidden[:, :640], hidden[:, 640:704]

    @pl.loop(0, 8)
    def _(n):
        at = pl.multiple_of(n * 256, 256)
        part = lax.dot_general(
            first,
            jnp.concatenate(
                [pieces[k, n * 2 + j] for j in range(2) for k in range(4)], axis=0
            ),
            NT,
            preferred_element_type=jnp.float32,
        ) + lax.dot_general(
            second,
            bands[pl.ds(at, 256), 1408:1472],
            NT,
            preferred_element_type=jnp.float32,
        )
        part = part.astype(jnp.bfloat16).reshape(4, 2, 32, 256)
        mine_ref[:, :, pl.ds(at, 256)] = jnp.where(core == 0, part[:, 0], part[:, 1])
        theirs_ref[:, :, pl.ds(at, 256)] = jnp.where(core == 0, part[:, 1], part[:, 0])


def ffn(core, after, gain, wide, pieces):
    half = jax.ShapeDtypeStruct((4, 32, 2048), jnp.bfloat16)
    return pl.pallas_call(
        ffn_kernel,
        out_shape=(half, half),
        in_specs=[
            whole(pltpu.SMEM),
            whole(pltpu.HBM),
            whole(),
            whole(pltpu.HBM),
            whole(pltpu.HBM),
        ],
        out_specs=(whole(), whole()),
        scratch_shapes=[
            pltpu.VMEM((2048, 1536), jnp.bfloat16),
            pltpu.VMEM((256, 2048), jnp.bfloat16),
            pltpu.VMEM((4, 16, 32, 640), jnp.bfloat16),
            pltpu.VMEM((256, 2048), jnp.bfloat16),
            pltpu.VMEM((256, 1408), jnp.float32),
            pltpu.VMEM((256, 768), jnp.bfloat16),
            pltpu.SemaphoreType.DMA((4,)),
        ],
        compiler_params=pltpu.CompilerParams(vmem_limit_bytes=52 * 2**20),
        cost_estimate=pl.CostEstimate(
            flops=2 * 256 * 2048 * 2112, bytes_accessed=11 * 2**20, transcendentals=256 * 704
        ),
        name="ffn",
    )(core, after, gain, wide, pieces)


def local(
    residual,
    queries,
    forget_gate_logits,
    projected_values,
    output_gate_logits,
    lower_bound_margin,
    extra_forget_logs,
    per_head_norm_gain,
    output_weight,
    feedforward_norm_gain,
    gate_weight,
    up_weight,
    down_weight,
):
    y = lax.axis_index("y").reshape(1)
    z = lax.axis_index("z").reshape(1)
    core = lax.axis_index("c")
    turned = down_weight.T
    out_rows, scaled, packed = scanned(
        queries,
        forget_gate_logits,
        projected_values,
        lower_bound_margin.reshape(1, HD),
        extra_forget_logs,
        gate_weight,
        up_weight,
        turned,
    )
    along_y = lax.all_gather(packed, "y")
    wide = lax.all_gather(along_y[:, :32].reshape(128, 1536), "z", axis=0, tiled=True)
    out_copies = jnp.broadcast_to(output_weight, (4, *output_weight.shape))
    out_mine = lax.all_to_all(out_copies, "x", split_axis=0, concat_axis=0, tiled=True)
    total, here = joined_over_y(y, along_y, turned)
    along_z = lax.all_gather(total.astype(jnp.float16), "z")
    own = (along_z[:, :32].astype(jnp.float32) * (1.0 / SCALE)).astype(jnp.bfloat16)
    own = jnp.broadcast_to(own, (4, 16, 32, 640))
    pieces = lax.all_to_all(own, "y", split_axis=0, concat_axis=0, tiled=True)
    lines = along_z[:, 32:].astype(jnp.float32)
    lines, out_mine = lax.optimization_barrier((lines, out_mine))
    out_other = shifted(out_mine, "c", 1)
    gated = mixed_rows(
        z,
        lines,
        here,
        out_rows,
        scaled,
        output_gate_logits,
        per_head_norm_gain.reshape(1, HD),
    )
    heads = lax.all_gather(gated, "x")
    heads_other = shifted(heads, "c", 1)
    projected = 0.0
    for part, weight in ((heads, out_mine), (heads_other, out_other)):
        projected = projected + jnp.dot(
            part.transpose(1, 0, 2).reshape(256, 512),
            weight.reshape(512, 2048),
            preferred_element_type=jnp.float32,
        )
    after_mixer = (residual.astype(jnp.float32) + projected).astype(jnp.bfloat16)
    gain = feedforward_norm_gain.reshape(1, 2048)
    mine, theirs = ffn(core.reshape(1), after_mixer, gain, wide, pieces)
    swapped = shifted(theirs, "c", 1)
    pair = (mine.astype(jnp.float32) + swapped.astype(jnp.float32)).astype(jnp.bfloat16)
    place = lax.axis_index(TP) * 32
    own_rows = lax.dynamic_slice_in_dim(after_mixer, place, 32, 0)
    pair, own_rows = lax.optimization_barrier((pair, own_rows))
    arrived = lax.all_to_all(pair, "x", split_axis=0, concat_axis=0, tiled=True)
    ffn_sum = arrived.astype(jnp.float32).sum(axis=0)
    finished = (own_rows.astype(jnp.float32) + 0.5 * ffn_sum).astype(jnp.bfloat16)
    copies = jnp.broadcast_to(finished, (4, 32, 2048))
    along_x = lax.all_to_all(copies, "x", split_axis=0, concat_axis=0, tiled=True)
    others = shifted(along_x, "c", 1)
    first = jnp.where(core == 0, along_x, others)
    second = jnp.where(core == 0, others, along_x)
    return jnp.stack([first, second], axis=1).reshape(256, 2048)


def solution(mesh):
    finer = Mesh(mesh.devices.reshape(16, 4, 4, 2), ("z", "y", "x", "c"))
    placed = (
        P(SP, None),
        P(SP, TP),
        P(SP, TP),
        P(SP, TP),
        P(SP, TP),
        P(TP),
        P(SP, TP),
        P(),
        P(TP, None),
        P(),
        P(SP, TP),
        P(SP, TP),
        P(TP, SP),
    )
    return jax.shard_map(
        local, mesh=finer, in_specs=placed, out_specs=P(SP, None), check_vma=False
    )
```

```python
import jax
import jax.numpy as jnp
from jax import lax
from jax.experimental import pallas as pl
from jax.experimental.pallas import tpu as pltpu
from jax.sharding import Mesh
from jax.sharding import PartitionSpec as P


HD = 128
BLOCK = 64
SP = ("z", "y")
TP = ("x", "c")
SCALE = 2.0**18
STATE_SCALE = 2.0**10
NN = (((1,), (0,)), ((), ()))
NT = (((1,), (1,)), ((), ()))
TN = (((0,), (0,)), ((), ()))


eps = 1e-06


def shifted(value, axis, step):
    size = lax.axis_size(axis)
    return lax.ppermute(value, axis, [(k, (k + step) % size) for k in range(size)])


def whole(space=pltpu.VMEM):
    return pl.BlockSpec(memory_space=space)


def dot(left, right, dims=NN):
    return lax.dot_general(
        left.astype(jnp.bfloat16),
        right.astype(jnp.bfloat16),
        dims,
        preferred_element_type=jnp.float32,
    )


def halves(value):
    high = value.astype(jnp.bfloat16)
    return high, (value - high.astype(jnp.float32)).astype(jnp.bfloat16)


def scan_kernel(
    q_ref,
    f_ref,
    v_ref,
    margin_ref,
    extra_ref,
    gate_ref,
    up_ref,
    out_ref,
    scaled_ref,
    packed_ref,
):
    queries = q_ref[...].astype(jnp.float32)
    inflow = margin_ref[...] * jax.nn.sigmoid(-f_ref[...].astype(jnp.float32))
    keep_log = jnp.log1p(-inflow) + extra_ref[...]
    row = lax.broadcasted_iota(jnp.int32, (256, 256), 0)
    column = lax.broadcasted_iota(jnp.int32, (256, 256), 1)
    lower = (column <= row).astype(jnp.float32)
    total = jnp.dot(
        lower, keep_log, precision=lax.Precision.HIGHEST, preferred_element_type=jnp.float32
    )
    scaled_ref[...] = (queries * jnp.exp(total)).astype(jnp.bfloat16)
    causal = lax.broadcasted_iota(jnp.int32, (BLOCK, BLOCK), 1) <= lax.broadcasted_iota(
        jnp.int32, (BLOCK, BLOCK), 0
    )
    state = None
    ended = jnp.zeros((1, HD), jnp.float32)
    for k in range(256 // BLOCK):
        rows = slice(k * BLOCK, (k + 1) * BLOCK)
        inside, sums = queries[rows], total[rows]
        middle, end = sums[BLOCK // 2 - 1 : BLOCK // 2], sums[BLOCK - 1 :]
        values = v_ref[rows]
        scores = dot(inside * jnp.exp(sums - middle), inflow[rows] * jnp.exp(middle - sums), NT)
        result = dot(jnp.where(causal, scores, 0.0), values)
        added = dot(values, inflow[rows] * jnp.exp(end - sums), TN)
        if state is not None:
            result = result + dot(inside * jnp.exp(sums - ended), state, NT)
            added = added + jnp.exp(end - ended) * state
        out_ref[rows, :] = result
        state, ended = added, end
    packed = state.astype(jnp.bfloat16)
    for k in range(8):
        packed_ref[32:, k * 128 : (k + 1) * 128] = packed[k * 16 : (k + 1) * 16]
    high, low = halves(jnp.broadcast_to(ended, (16, HD)))
    packed_ref[32:, 1024:1152] = high
    packed_ref[32:, 1152:1280] = low
    packed_ref[32:, 1280:] = jnp.zeros((16, 128), jnp.bfloat16)
    for k in range(5):
        packed_ref[:32, k * 256 : k * 256 + 128] = gate_ref[:, k * 128 : (k + 1) * 128]
        packed_ref[:32, k * 256 + 128 : (k + 1) * 256] = up_ref[:, k * 128 : (k + 1) * 128]
    packed_ref[:32, 1280:1408] = jnp.concatenate([gate_ref[:, 640:], up_ref[:, 640:]], axis=1)


def scanned(*operands):
    return pl.pallas_call(
        scan_kernel,
        out_shape=(
            jax.ShapeDtypeStruct((256, HD), jnp.float32),
            jax.ShapeDtypeStruct((256, HD), jnp.bfloat16),
            jax.ShapeDtypeStruct((48, 1408), jnp.bfloat16),
        ),
        in_specs=[whole()] * 7,
        out_specs=(whole(),) * 3,
        cost_estimate=pl.CostEstimate(
            flops=4_000_000_000, bytes_accessed=500_000, transcendentals=300_000
        ),
        name="scan",
    )(*operands)


def y_kernel(y_ref, pieces_ref, turned_ref, total_ref, here_ref):
    y = y_ref[0]
    total_sum = here_sum = jnp.zeros((1, HD), jnp.float32)
    total = here = jnp.zeros((HD, HD), jnp.float32)
    for k in range(4):
        here = jnp.where(k == y, total, here)
        here_sum = jnp.where(k == y, total_sum, here_sum)
        state = jnp.concatenate(
            [pieces_ref[k, 32:, j * 128 : (j + 1) * 128] for j in range(8)], axis=0
        ).astype(jnp.float32)
        one = pieces_ref[k, 32:, 1024:1152].astype(jnp.float32)[:1]
        one = one + pieces_ref[k, 32:, 1152:1280].astype(jnp.float32)[:1]
        total = jnp.exp(one) * total + state
        total_sum = total_sum + one
    here_ref[:HD, :] = here
    here_ref[HD:, :] = jnp.broadcast_to(here_sum, (8, HD))
    total_ref[:32, :704] = turned_ref[...].astype(jnp.float32) * SCALE
    total_ref[:32, 704:] = jnp.zeros((32, 64), jnp.float32)
    for k in range(4):
        total_ref[32:, k * 128 : (k + 1) * 128] = total[k * 32 : (k + 1) * 32] * STATE_SCALE
    total_ref[32:, 512:640] = jnp.broadcast_to(total_sum, (32, HD))
    total_ref[32:, 640:] = jnp.zeros((32, HD), jnp.float32)


def joined_over_y(y, pieces, turned):
    return pl.pallas_call(
        y_kernel,
        out_shape=(
            jax.ShapeDtypeStruct((64, 768), jnp.float32),
            jax.ShapeDtypeStruct((136, HD), jnp.float32),
        ),
        in_specs=[whole(pltpu.SMEM), whole(), whole()],
        out_specs=(whole(), whole()),
        cost_estimate=pl.CostEstimate(
            flops=1_000_000_000, bytes_accessed=700_000, transcendentals=1000
        ),
        name="join",
    )(y, pieces, turned)


def mix_kernel(z_ref, lines_ref, here_ref, out_ref, scaled_ref, logits_ref, gain_ref, gated_ref):
    z = z_ref[0]
    before = jnp.zeros((HD, HD), jnp.float32)
    for k in range(15):
        state = jnp.concatenate(
            [lines_ref[k, :, j * 128 : (j + 1) * 128] for j in range(4)], axis=0
        )
        joined = jnp.exp(lines_ref[k, :1, 512:640]) * before + state
        before = jnp.where(k < z, joined, before)
    here = here_ref[...]
    state = jnp.exp(here[HD : HD + 1]) * (before * (1.0 / STATE_SCALE)) + here[:HD]
    mixed = out_ref[...] + dot(scaled_ref[...], state, NT)
    normed = mixed * lax.rsqrt(jnp.mean(mixed * mixed, axis=-1, keepdims=True) + eps)
    logits = logits_ref[...].astype(jnp.float32)
    gated = (normed * gain_ref[...] * (logits * jax.nn.sigmoid(logits))).astype(jnp.bfloat16)
    gated_ref[...] = gated


def mixed_rows(z, lines, here, out, scaled, logits, gain):
    return pl.pallas_call(
        mix_kernel,
        out_shape=jax.ShapeDtypeStruct((256, HD), jnp.bfloat16),
        in_specs=[whole(pltpu.SMEM)] + [whole()] * 6,
        out_specs=whole(),
        cost_estimate=pl.CostEstimate(
            flops=2_000_000_000, bytes_accessed=2_000_000, transcendentals=100_000
        ),
        name="mix",
    )(z, lines, here, out, scaled, logits, gain)


def ffn_kernel(
    core_ref,
    after_ref,
    gain_ref,
    wide_ref,
    pieces_ref,
    mine_ref,
    theirs_ref,
    bands,
    after_rows,
    pieces,
    normed,
    half,
    hidden,
    band_sems,
):
    core = core_ref[0]
    band_copies = [
        pltpu.make_async_copy(
            wide_ref.at[pl.ds(start, size)], bands.at[pl.ds(start, size)], band_sems.at[n]
        )
        for n, (start, size) in enumerate(((0, 512), (512, 1536)))
    ]
    after_copy = pltpu.make_async_copy(after_ref, after_rows, band_sems.at[2])
    piece_copy = pltpu.make_async_copy(pieces_ref, pieces, band_sems.at[3])
    after_copy.start()
    for copy in band_copies:
        copy.start()
    piece_copy.start()
    after_copy.wait()
    for k in range(8):
        lines = slice(k * 32, (k + 1) * 32)
        after = after_rows[lines].astype(jnp.float32)
        scale = lax.rsqrt(jnp.mean(after * after, axis=-1, keepdims=True) + eps)
        normed[lines] = (after * scale * gain_ref[...]).astype(jnp.bfloat16)
    spans = [slice(n * 256, min(n * 256 + 256, 1408)) for n in range(6)]
    rows = normed[:, :512]
    band_copies[0].wait()
    for span in spans:
        half[:, span] = jnp.dot(rows, bands[:512, span], preferred_element_type=jnp.float32)
    rows = normed[:, 512:]
    band_copies[1].wait()
    for n, span in enumerate(spans):
        both = half[:, span] + jnp.dot(
            rows, bands[512:, span], preferred_element_type=jnp.float32
        )
        width = both.shape[1] // 2
        gate, up = both[:, :width], both[:, width:]
        hidden[:, n * 128 : n * 128 + width] = (gate * jax.nn.sigmoid(gate) * up).astype(
            jnp.bfloat16
        )
    piece_copy.wait()
    inner = hidden[:, :704]

    @pl.loop(0, 8)
    def _(n):
        at = pl.multiple_of(n * 256, 256)
        part = lax.dot_general(
            inner,
            jnp.concatenate(
                [pieces[k, n * 2 + j, :, :704] for j in range(2) for k in range(4)], axis=0
            ),
            NT,
            preferred_element_type=jnp.float32,
        )
        part = part.astype(jnp.bfloat16).reshape(4, 2, 32, 256)
        mine_ref[:, :, pl.ds(at, 256)] = jnp.where(core == 0, part[:, 0], part[:, 1])
        theirs_ref[:, :, pl.ds(at, 256)] = jnp.where(core == 0, part[:, 1], part[:, 0])


def ffn(core, after, gain, wide, pieces):
    half = jax.ShapeDtypeStruct((4, 32, 2048), jnp.bfloat16)
    return pl.pallas_call(
        ffn_kernel,
        out_shape=(half, half),
        in_specs=[
            whole(pltpu.SMEM),
            whole(pltpu.HBM),
            whole(),
            whole(pltpu.HBM),
            whole(pltpu.HBM),
        ],
        out_specs=(whole(), whole()),
        scratch_shapes=[
            pltpu.VMEM((2048, 1408), jnp.bfloat16),
            pltpu.VMEM((256, 2048), jnp.bfloat16),
            pltpu.VMEM((4, 16, 32, 768), jnp.bfloat16),
            pltpu.VMEM((256, 2048), jnp.bfloat16),
            pltpu.VMEM((256, 1408), jnp.float32),
            pltpu.VMEM((256, 768), jnp.bfloat16),
            pltpu.SemaphoreType.DMA((4,)),
        ],
        compiler_params=pltpu.CompilerParams(vmem_limit_bytes=52 * 2**20),
        cost_estimate=pl.CostEstimate(
            flops=2 * 256 * 2048 * 2112, bytes_accessed=11 * 2**20, transcendentals=256 * 704
        ),
        name="ffn",
    )(core, after, gain, wide, pieces)


def local(
    residual,
    queries,
    forget_gate_logits,
    projected_values,
    output_gate_logits,
    lower_bound_margin,
    extra_forget_logs,
    per_head_norm_gain,
    output_weight,
    feedforward_norm_gain,
    gate_weight,
    up_weight,
    down_weight,
):
    y = lax.axis_index("y").reshape(1)
    z = lax.axis_index("z").reshape(1)
    core = lax.axis_index("c")
    turned = down_weight.T
    out_rows, scaled, packed = scanned(
        queries,
        forget_gate_logits,
        projected_values,
        lower_bound_margin.reshape(1, HD),
        extra_forget_logs,
        gate_weight,
        up_weight,
    )
    along_y = lax.all_gather(packed, "y")
    wide = lax.all_gather(along_y[:, :32].reshape(128, 1408), "z", axis=0, tiled=True)
    out_copies = jnp.broadcast_to(output_weight, (4, *output_weight.shape))
    out_mine = lax.all_to_all(out_copies, "x", split_axis=0, concat_axis=0, tiled=True)
    total, here = joined_over_y(y, along_y, turned)
    along_z = lax.all_gather(total.astype(jnp.float16), "z")
    own = (along_z[:, :32].astype(jnp.float32) * (1.0 / SCALE)).astype(jnp.bfloat16)
    own = jnp.broadcast_to(own, (4, 16, 32, 768))
    pieces = lax.all_to_all(own, "y", split_axis=0, concat_axis=0, tiled=True)
    lines = along_z[:, 32:].astype(jnp.float32)
    lines, out_mine = lax.optimization_barrier((lines, out_mine))
    out_other = shifted(out_mine, "c", 1)
    gated = mixed_rows(
        z,
        lines,
        here,
        out_rows,
        scaled,
        output_gate_logits,
        per_head_norm_gain.reshape(1, HD),
    )
    heads = lax.all_gather(gated, "x")
    heads_other = shifted(heads, "c", 1)
    projected = 0.0
    for part, weight in ((heads, out_mine), (heads_other, out_other)):
        projected = projected + jnp.dot(
            part.transpose(1, 0, 2).reshape(256, 512),
            weight.reshape(512, 2048),
            preferred_element_type=jnp.float32,
        )
    after_mixer = (residual.astype(jnp.float32) + projected).astype(jnp.bfloat16)
    gain = feedforward_norm_gain.reshape(1, 2048)
    mine, theirs = ffn(core.reshape(1), after_mixer, gain, wide, pieces)
    swapped = shifted(theirs, "c", 1)
    pair = (mine.astype(jnp.float32) + swapped.astype(jnp.float32)).astype(jnp.bfloat16)
    place = lax.axis_index(TP) * 32
    own_rows = lax.dynamic_slice_in_dim(after_mixer, place, 32, 0)
    pair, own_rows = lax.optimization_barrier((pair, own_rows))
    arrived = lax.all_to_all(pair, "x", split_axis=0, concat_axis=0, tiled=True)
    ffn_sum = arrived.astype(jnp.float32).sum(axis=0)
    finished = (own_rows.astype(jnp.float32) + 0.5 * ffn_sum).astype(jnp.bfloat16)
    copies = jnp.broadcast_to(finished, (4, 32, 2048))
    along_x = lax.all_to_all(copies, "x", split_axis=0, concat_axis=0, tiled=True)
    others = shifted(along_x, "c", 1)
    first = jnp.where(core == 0, along_x, others)
    second = jnp.where(core == 0, others, along_x)
    return jnp.stack([first, second], axis=1).reshape(256, 2048)


def solution(mesh):
    finer = Mesh(mesh.devices.reshape(16, 4, 4, 2), ("z", "y", "x", "c"))
    placed = (
        P(SP, None),
        P(SP, TP),
        P(SP, TP),
        P(SP, TP),
        P(SP, TP),
        P(TP),
        P(SP, TP),
        P(),
        P(TP, None),
        P(),
        P(SP, TP),
        P(SP, TP),
        P(TP, SP),
    )
    return jax.shard_map(
        local, mesh=finer, in_specs=placed, out_specs=P(SP, None), check_vma=False
    )
```
